32 devices in a mesh: sp: 8 (over z, y), tp: 4 (over x, core).
Axes of the slice: x: 2, y: 2, z: 4, core: 2. Of those that a mesh axis runs over, the one named last changes fastest.
Arguments:
- inputs: bfloat16 [12288, 2048], P('sp'), may hold values from -6 to 6
- norm_gain: float32 [2048], replicated, may hold values from 0.1 to 1.9
- pool_weight: bfloat16 [2048, 1024], P(None, 'tp'), may hold values from -0.125 to 0.125
- query_weight: bfloat16 [2048, 1024], P(None, 'tp'), may hold values from -0.125 to 0.125
- forget_weight: bfloat16 [2048, 1024], P(None, 'tp'), may hold values from -0.125 to 0.125
- value_weight: bfloat16 [2048, 1024], P(None, 'tp'), may hold values from -0.125 to 0.125
- outgate_weight: bfloat16 [2048, 1024], P(None, 'tp'), may hold values from -0.125 to 0.125
- pool_mix: bfloat16 [4, 256, 256], P('tp'), may hold values from -0.375 to 0.375
- pool_scale: float32 [1024], P('tp'), may hold values from 0.1 to 1.9
- lower_bound: float32 [1024], P('tp'), may hold values from 0.9 to 1
- extra_decay: float32 [12288, 8], P('sp', 'tp'), may hold values from -1 to 0
- recur_gain: float32 [1024], P('tp'), may hold values from 0.1 to 1.9
- init_state: float32 [8, 128, 128], P('tp'), may hold values from -0.013531647 to 0.013531647
- out_pool: bfloat16 [1024, 2048], P('tp'), may hold values from -0.125 to 0.125
- out_recur: bfloat16 [1024, 2048], P('tp'), may hold values from -0.125 to 0.125
Outputs:
- mixed: bfloat16 [12288, 2048], P(('sp', 'tp'))
The draws below stay inside these ranges and needn't reach their ends.
All inputs are finite; a program needn't handle non-finite values.
Results may differ from the reference program's by a relative error of at most 0.014.
Values may be sent and summed in bfloat16 or wider, within the bound.
No kernel may reach another device: no remote copies, remote signals or barrier semaphores. Data moves between devices by JAX's collectives and lax.ppermute only.
A program may use at most 128 MiB of HBM per device.

```python
import jax
import jax.numpy as jnp
from jax import lax

D = 2048
BRANCH = 1024
GROUPS = 4
HEAD_K = 128
BLOCK = 64
TOK_DEV = 1536
GROUP_W = 256
HEADS = 8
SEQUENCE_LENGTH = 12288


def draw_lower_bound(key, part):
    count_of_heads = BRANCH // HEAD_K
    key_slow, key_fast, key_pick = jax.random.split(jax.random.fold_in(key, 11), 3)
    slow_gap = jnp.exp(jax.random.uniform(key_slow, (BRANCH,), jnp.float32, jnp.log(0.15), 0.0)) / SEQUENCE_LENGTH
    fast_head = jax.random.bernoulli(key_pick, 0.5, (count_of_heads,))
    fast_gap = jnp.exp(jax.random.uniform(key_fast, (BRANCH,), jnp.float32, jnp.log(0.03), jnp.log(0.08)))
    fast_channel = jnp.repeat(fast_head, HEAD_K)
    gap = jnp.where(fast_channel, fast_gap, slow_gap)
    return (1.0 - gap).astype(jnp.float32)


def draw_extra_decay(key, part):
    count_of_heads = BRANCH // HEAD_K
    key_rate, key_location, key_depth = jax.random.split(jax.random.fold_in(key, 23), 3)
    span_count = SEQUENCE_LENGTH // TOK_DEV
    rate = jnp.exp(jax.random.uniform(key_rate, (span_count, count_of_heads), jnp.float32, jnp.log(0.1), jnp.log(0.6)))
    base_offset = -jnp.repeat(rate, TOK_DEV, axis=0) / SEQUENCE_LENGTH
    spurt_rows = jax.random.randint(key_location, (2, count_of_heads), 0, SEQUENCE_LENGTH)
    layer_depth = jnp.log(jax.random.uniform(key_depth, (2, count_of_heads), jnp.float32, 0.55, 0.8))
    token_positions = jnp.arange(SEQUENCE_LENGTH, dtype=jnp.int32)[:, None, None]
    spurt_list = jnp.sum(jnp.where(token_positions == spurt_rows[None], layer_depth[None], 0.0), axis=1)
    return (base_offset + spurt_list).astype(jnp.float32)


def steps_of(rng, extent, cuts, low, high):
    level, own = 1.0, jax.random.fold_in(rng, 6)
    for position, shards_of in cuts:
        draws = jnp.exp(jax.random.uniform(jax.random.fold_in(own, position), (shards_of,), jnp.float32, low / len(cuts), high / len(cuts)))
        level = level * jnp.repeat(draws, extent[position] // shards_of).reshape([-1 if axis == position else 1 for axis in range(len(extent))])
    return level


def noise(own_key, shape, deviation, limit, cuts=(), kind=jnp.bfloat16):
    drawn = jax.random.normal(own_key, shape, jnp.float32) * deviation
    if len(cuts) > 0:
        drawn = steps_of(own_key, shape, cuts, -0.22, 0.18) * drawn
    return jnp.clip(drawn, min=-limit, max=limit).astype(kind)


def setup_inputs(seed: int = 0) -> dict:
    splits = jax.random.split(jax.random.key(seed), 16)
    inputs = noise(splits[0], (SEQUENCE_LENGTH, D), 1.0, 6.0, ((0, 8),))
    norm_gain = jnp.clip(1.0 + 0.18 * jax.random.normal(splits[1], (D,), jnp.float32), 0.1, 1.9)
    pool_weight = noise(splits[2], (D, BRANCH), D ** -0.5, 0.125, ((1, 4),))
    query_weight = noise(splits[3], (D, BRANCH), D ** -0.5, 0.125, ((1, 4),))
    forget_weight = noise(splits[4], (D, BRANCH), D ** -0.5, 0.125, ((1, 4),))
    value_weight = noise(splits[5], (D, BRANCH), D ** -0.5, 0.125, ((1, 4),))
    outgate_weight = noise(splits[6], (D, BRANCH), D ** -0.5, 0.125, ((1, 4),))
    pool_mix = noise(splits[7], (GROUPS, GROUP_W, GROUP_W), GROUP_W ** -0.5, 0.375, ((0, 4),))
    pool_scale = jnp.clip(1.0 + 0.18 * jax.random.normal(splits[8], (BRANCH,), jnp.float32), 0.1, 1.9)
    lower_bound = draw_lower_bound(jax.random.fold_in(splits[15], 71), 0)
    extra_decay = draw_extra_decay(jax.random.fold_in(splits[15], 71), 0)
    recur_gain = jnp.clip(1.0 + 0.18 * jax.random.normal(splits[11], (BRANCH,), jnp.float32), 0.1, 1.9)
    init_state = noise(splits[12], (HEADS, HEAD_K, HEAD_K), (0.25 * SEQUENCE_LENGTH ** -0.5), 0.013531647, ((0, 4),), jnp.float32)
    out_pool = noise(splits[13], (BRANCH, D), (2 * BRANCH) ** -0.5, 0.125, ((0, 4),))
    out_recur = noise(splits[14], (BRANCH, D), (2 * BRANCH) ** -0.5, 0.125, ((0, 4),))
    return dict(inputs=inputs, norm_gain=norm_gain, pool_weight=pool_weight, query_weight=query_weight, forget_weight=forget_weight, value_weight=value_weight, outgate_weight=outgate_weight, pool_mix=pool_mix, pool_scale=pool_scale, lower_bound=lower_bound, extra_decay=extra_decay, recur_gain=recur_gain, init_state=init_state, out_pool=out_pool, out_recur=out_recur)


norm_eps = 1e-05
top_precision = lax.Precision.HIGHEST

def norm_rows(array, scale_vec):
    widened = array.astype(jnp.float32)
    scaled = widened * lax.rsqrt(lax.optimization_barrier(jnp.mean(widened * widened, axis=-1, keepdims=True)) + norm_eps)
    return (scaled * scale_vec).astype(jnp.bfloat16)

def window_sums(widened):
    results = []
    current = widened
    for level_idx in range(GROUPS):
        stride = 2 ** level_idx
        shifted = jnp.pad(current, ((stride, 0), (0, 0)))[:current.shape[0]]
        current = current + shifted
        results.append(current)
    return results

def pool_branch(pool_in, pool_mix, pool_scale):
    row_count = pool_in.shape[0]
    group_width = pool_mix.shape[1]
    widened = pool_in.astype(jnp.float32)
    window_totals = window_sums(widened)
    token_positions = jnp.arange(row_count, dtype=jnp.int32)
    pieces = []
    for group_idx in range(pool_mix.shape[0]):
        columns = slice(group_idx * group_width, (group_idx + 1) * group_width)
        reach = jnp.minimum(token_positions + 1, 2 ** (group_idx + 1)).astype(jnp.float32)
        pieces.append(window_totals[group_idx][:, columns] / reach[:, None] - widened[:, columns])
    pooled = jnp.stack(pieces, axis=1).astype(jnp.bfloat16)
    mixed_groups = jnp.einsum('rgc,gcd->rgd', pooled.astype(jnp.float32), pool_mix.astype(jnp.float32))
    return (mixed_groups.reshape(row_count, -1) * pool_scale).astype(jnp.bfloat16)

def recur_inputs(query_raw, forget_raw, value_raw, bound_vec, extra_log, head_k, block_len):
    row_count = query_raw.shape[0]
    count_of_heads = query_raw.shape[1] // head_k
    block_count = row_count // block_len
    forget_pre = forget_raw.astype(jnp.float32)
    log_f = jnp.logaddexp(jnp.log(bound_vec), jnp.log1p(-bound_vec) + jax.nn.log_sigmoid(forget_pre))
    log_f = log_f.reshape(row_count, count_of_heads, head_k) + extra_log[:, :, None]
    key_input = ((1.0 - bound_vec) * jax.nn.sigmoid(-forget_pre)).reshape(row_count, count_of_heads, head_k)
    query_input = jax.nn.silu(query_raw.astype(jnp.float32)).reshape(row_count, count_of_heads, head_k)
    value_input = value_raw.astype(jnp.float32).reshape(row_count, count_of_heads, head_k)

    def to_blocks(array):
        return array.reshape(block_count, block_len, count_of_heads, head_k).transpose(2, 0, 1, 3)
    return (to_blocks(query_input), to_blocks(key_input), to_blocks(value_input), to_blocks(log_f))

def block_parts(query_input, key_input, value_input, log_f):
    block_len = log_f.shape[2]
    cum_log = jnp.cumsum(log_f, axis=2)
    last_log = cum_log[:, :, -1:, :]
    query_dec = query_input * jnp.exp(cum_log)
    key_dec = key_input * jnp.exp(-cum_log)
    scores = jnp.einsum('hntk,hnsk->hnts', query_dec, key_dec, precision=top_precision)
    causal = jnp.tril(jnp.ones((block_len, block_len), dtype=bool))
    scores = jnp.where(causal, scores, 0.0)
    within = jnp.einsum('hnts,hnsv->hntv', scores, value_input, precision=top_precision)
    contrib = jnp.einsum('hnsk,hnsv->hnkv', key_input * jnp.exp(last_log - cum_log), value_input, precision=top_precision)
    decays = jnp.exp(last_log[:, :, 0, :])
    return (query_dec, within, decays, contrib)

def chain(earlier, later_part):
    return (earlier[0] * later_part[0], later_part[0][..., None] * earlier[1] + later_part[1])

def recur_branch(query_raw, forget_raw, value_raw, outgate_raw, bound_vec, extra_log, recur_gain, init_state):
    row_count = query_raw.shape[0]
    head_k = init_state.shape[1]
    count_of_heads = init_state.shape[0]
    query_in, key_in, value_in, log_f = recur_inputs(query_raw, forget_raw, value_raw, bound_vec, extra_log, head_k, BLOCK)
    query_dec, within, decays, contrib = block_parts(query_in, key_in, value_in, log_f)
    running = lax.associative_scan(chain, (decays, contrib), axis=1)
    enter_a = jnp.concatenate([jnp.ones_like(decays[:, :1]), running[0][:, :-1]], axis=1)
    enter_s = jnp.concatenate([jnp.zeros_like(contrib[:, :1]), running[1][:, :-1]], axis=1)
    state_in = enter_s + enter_a[..., None] * init_state[:, None]
    recur_out = within + jnp.einsum('hntk,hnkv->hntv', query_dec, state_in, precision=top_precision)
    recur_out = recur_out.transpose(1, 2, 0, 3).reshape(row_count, count_of_heads, head_k)
    recur_out = recur_out * lax.rsqrt(lax.optimization_barrier(jnp.mean(recur_out * recur_out, axis=-1, keepdims=True)) + norm_eps)
    recur_out = recur_out * recur_gain.reshape(count_of_heads, head_k)
    gated = recur_out.reshape(row_count, count_of_heads * head_k) * jax.nn.silu(outgate_raw.astype(jnp.float32))
    return gated.astype(jnp.bfloat16)

def reference(inputs, norm_gain, pool_weight, query_weight, forget_weight, value_weight, outgate_weight, pool_mix, pool_scale, lower_bound, extra_decay, recur_gain, init_state, out_pool, out_recur):
    normed = norm_rows(inputs, norm_gain)
    pool_in = jnp.dot(normed, pool_weight, preferred_element_type=jnp.float32).astype(jnp.bfloat16)
    query_raw = jnp.dot(normed, query_weight, preferred_element_type=jnp.float32).astype(jnp.bfloat16)
    forget_raw = jnp.dot(normed, forget_weight, preferred_element_type=jnp.float32).astype(jnp.bfloat16)
    value_raw = jnp.dot(normed, value_weight, preferred_element_type=jnp.float32).astype(jnp.bfloat16)
    outgate_raw = jnp.dot(normed, outgate_weight, preferred_element_type=jnp.float32).astype(jnp.bfloat16)
    y_pool = pool_branch(pool_in, pool_mix, pool_scale)
    y_recur = recur_branch(query_raw, forget_raw, value_raw, outgate_raw, lower_bound, extra_decay, recur_gain, init_state)
    summed = jnp.dot(y_pool, out_pool, preferred_element_type=jnp.float32)
    summed = summed + jnp.dot(y_recur, out_recur, preferred_element_type=jnp.float32)
    return summed.astype(jnp.bfloat16)
```

```python
import functools

import jax
import jax.numpy as jnp
from jax import lax
from jax.experimental import pallas as pl
from jax.experimental.pallas import tpu as pltpu
from jax.sharding import PartitionSpec as P

norm_eps = 1e-05
halo_rows = 16
chunk = 128
msg_pad = 16
f32 = jnp.float32
bf16 = jnp.bfloat16


def dot(a, b, dims=((1,), (0,))):
    return lax.dot_general(a, b, (dims, ((), ())), preferred_element_type=f32)


def norm_block(x, gain):
    wide = x.astype(f32)
    mean = jnp.mean(wide * wide, axis=-1, keepdims=True)
    return (wide * lax.rsqrt(mean + norm_eps) * gain).astype(bf16)


def sigmoid(x):
    return 1.0 / (1.0 + jnp.exp(-x))


def lower_triangle(size):
    row = lax.broadcasted_iota(jnp.int32, (size, size), 0)
    col = lax.broadcasted_iota(jnp.int32, (size, size), 1)
    return row >= col


def state_kernel(
    x_ref, gain_ref, fw_ref, vw_ref, lb_ref, extra_ref,
    normed_ref, key_ref, decay_ref, value_ref, start_ref, rows_ref, msg_ref,
    state, total,
):
    step = pl.program_id(0)
    heads, head_k = state.shape[0], state.shape[1]
    tile = x_ref.shape[0]

    @pl.when(step == 0)
    def _():
        state[...] = jnp.zeros_like(state)
        total[...] = jnp.zeros_like(total)

    normed = norm_block(x_ref[...], gain_ref[...])
    normed_ref[...] = normed
    forget = dot(normed, fw_ref[...])
    value = dot(normed, vw_ref[...]).astype(bf16)
    value_ref[...] = value
    gap = 1.0 - lb_ref[...]
    key = gap / (1.0 + jnp.exp(forget))
    extra = extra_ref[...]
    spread = jnp.concatenate(
        [jnp.broadcast_to(extra[:, h : h + 1], (tile, head_k)) for h in range(heads)], axis=1
    )
    log_f = jnp.log(1.0 - key) + spread
    high = log_f.astype(bf16)
    low = (log_f - high.astype(f32)).astype(bf16)
    triangle = lower_triangle(chunk).astype(f32).astype(bf16)
    for c in range(tile // chunk):
        span = slice(c * chunk, (c + 1) * chunk)
        cum = dot(triangle, high[span]) + dot(triangle, low[span])
        middle = cum[chunk // 2 - 1 : chunk // 2]
        last = cum[chunk - 1 :]
        decay_ref[span, :] = jnp.exp(cum - middle)
        key_dec = key[span] * jnp.exp(middle - cum)
        key_ref[span, :] = key_dec.astype(bf16)
        key_end = (key_dec * jnp.exp(last - middle)).astype(bf16)
        before = total[...]
        rows_ref[c] = jnp.concatenate(
            [jnp.exp(middle), jnp.exp(before), jnp.zeros((6, middle.shape[1]), f32)], axis=0
        )
        total[...] = before + last
        whole = jnp.exp(last)
        for h in range(heads):
            lanes = slice(h * head_k, (h + 1) * head_k)
            old = state[h]
            start_ref[c, h] = old.astype(bf16)
            contrib = dot(value[span, lanes], key_end[:, lanes], ((0,), (0,)))
            state[h] = old * whole[:, lanes] + contrib

    @pl.when(step == pl.num_programs(0) - 1)
    def _():
        decay = jnp.exp(total[...])
        high_part = decay.astype(bf16)
        low_part = (decay - high_part.astype(f32)).astype(bf16)
        for h in range(heads):
            lanes = slice(h * head_k, (h + 1) * head_k)
            msg_ref[h, :head_k, :] = state[h].astype(bf16)
            msg_ref[h, head_k:, :] = jnp.concatenate(
                [
                    high_part[:, lanes].astype(f32),
                    low_part[:, lanes].astype(f32),
                    jnp.zeros((msg_pad - 2, head_k), f32),
                ],
                axis=0,
            ).astype(bf16)


def local_kernel(
    place_ref, normed_ref, halo_ref, gain_ref, qw_ref, ow_ref, pw_ref, mix_ref, scale_ref,
    recur_gain_ref, key_ref, decay_ref, value_ref, start_ref, rows_ref,
    local_ref, qtot_ref, gate_ref, ypool_ref,
    tail, band,
):
    step = pl.program_id(0)
    tile = normed_ref.shape[0]
    head_k = start_ref.shape[-1]
    heads = start_ref.shape[1]
    first_pos = place_ref[0]
    window = place_ref[1]

    @pl.when(step == 0)
    def _():
        tail[...] = dot(norm_block(halo_ref[...], gain_ref[...]), pw_ref[...]).astype(bf16)
        row = lax.broadcasted_iota(jnp.int32, band.shape, 0)
        col = lax.broadcasted_iota(jnp.int32, band.shape, 1) - halo_rows
        back = row - col
        band[...] = ((back >= 0) & (back < window)).astype(f32).astype(bf16)

    normed = normed_ref[...]
    query = dot(normed, qw_ref[...])
    outgate = dot(normed, ow_ref[...])
    pool_in = dot(normed, pw_ref[...]).astype(bf16)
    gate_ref[...] = outgate * sigmoid(outgate) * recur_gain_ref[...]
    query = query * sigmoid(query)
    causal = lower_triangle(chunk)
    before = tail[...]
    for c in range(tile // chunk):
        span = slice(c * chunk, (c + 1) * chunk)
        part = pool_in[span]
        sums = dot(band[...], jnp.concatenate([before, part], axis=0))
        before = part[chunk - halo_rows :]
        position = (
            first_pos + step * tile + c * chunk
            + lax.broadcasted_iota(jnp.int32, (chunk, 1), 0)
        )
        count = jnp.minimum(position + 1, window).astype(f32)
        pooled = (sums / count - part.astype(f32)).astype(bf16)
        ypool_ref[span, :] = (dot(pooled, mix_ref[0]) * scale_ref[...]).astype(bf16)

        query_dec = query[span] * decay_ref[span, :]
        query_low = query_dec.astype(bf16)
        query_abs = query_dec * rows_ref[c, 0:1, :]
        qtot_ref[span, :] = (query_abs * rows_ref[c, 1:2, :]).astype(bf16)
        query_abs = query_abs.astype(bf16)
        for h in range(heads):
            lanes = slice(h * head_k, (h + 1) * head_k)
            scores = dot(query_low[:, lanes], key_ref[span, lanes], ((1,), (1,)))
            scores = jnp.where(causal, scores, 0.0).astype(bf16)
            within = dot(scores, value_ref[span, lanes])
            earlier = dot(query_abs[:, lanes], start_ref[c, h], ((1,), (1,)))
            local_ref[span, lanes] = within + earlier
    tail[...] = before


def output_kernel(
    place_ref, msgs_ref, init_ref, local_ref, qtot_ref, gate_ref, y_ref, carried
):
    head_k = init_ref.shape[-1]
    heads = init_ref.shape[0]
    devices = msgs_ref.shape[0]
    me = place_ref[2]

    @pl.when(pl.program_id(0) == 0)
    def _():
        for h in range(heads):
            def step(i, state):
                decay = (
                    msgs_ref[i, h, head_k : head_k + 1, :].astype(f32)
                    + msgs_ref[i, h, head_k + 1 : head_k + 2, :].astype(f32)
                )
                return state * decay + msgs_ref[i, h, :head_k, :].astype(f32)

            carried[h] = lax.fori_loop(0, me, step, init_ref[h].T).astype(bf16)

    for h in range(heads):
        lanes = slice(h * head_k, (h + 1) * head_k)
        recur = local_ref[:, lanes] + dot(qtot_ref[:, lanes], carried[h], ((1,), (1,)))
        mean = jnp.mean(recur * recur, axis=-1, keepdims=True)
        y_ref[:, lanes] = (recur * lax.rsqrt(mean + norm_eps) * gate_ref[:, lanes]).astype(bf16)


def fixed(*shape):
    return pl.BlockSpec(shape, lambda *_: (0,) * len(shape))


def moving(*shape):
    return pl.BlockSpec(shape, lambda i, *_: (i,) + (0,) * (len(shape) - 1))


limits = pltpu.CompilerParams(
    dimension_semantics=("arbitrary",), vmem_limit_bytes=56 * 1024 * 1024
)


def swapped(array, axis, bit):
    devices = lax.axis_size(axis)
    return lax.ppermute(array, axis, [(i, i ^ bit) for i in range(devices)])


def per_device(
    inputs, norm_gain, pool_weight, query_weight, forget_weight, value_weight, outgate_weight,
    pool_mix, pool_scale, lower_bound, extra_decay, recur_gain, init_state, out_pool, out_recur,
):
    rows, width = inputs.shape
    heads, head_k = init_state.shape[:2]
    channels = query_weight.shape[1]
    sp, tp = lax.axis_size("sp"), lax.axis_size("tp")
    sp_index, tp_index = lax.axis_index("sp"), lax.axis_index("tp")
    tile = 2 * chunk
    steps, chunks = rows // tile, tile // chunk
    gain = norm_gain[None]

    halo = lax.ppermute(
        inputs[rows - halo_rows :], "sp", [(i, i + 1) for i in range(sp - 1)]
    )
    sds = jax.ShapeDtypeStruct
    normed, key_dec, decay, value, starts, row_info, msg = pl.pallas_call(
        state_kernel,
        grid=(steps,),
        in_specs=[
            moving(tile, width), fixed(1, width), fixed(width, channels), fixed(width, channels),
            fixed(1, channels), moving(tile, heads),
        ],
        out_specs=[
            moving(tile, width), moving(tile, channels), moving(tile, channels),
            moving(tile, channels), moving(chunks, heads, head_k, head_k),
            moving(chunks, 8, channels), fixed(heads, head_k + msg_pad, head_k),
        ],
        out_shape=[
            sds((rows, width), bf16), sds((rows, channels), bf16), sds((rows, channels), f32),
            sds((rows, channels), bf16), sds((rows // chunk, heads, head_k, head_k), bf16),
            sds((rows // chunk, 8, channels), f32), sds((heads, head_k + msg_pad, head_k), bf16),
        ],
        scratch_shapes=[pltpu.VMEM((heads, head_k, head_k), f32), pltpu.VMEM((1, channels), f32)],
        compiler_params=limits,
        name="state_kernel",
    )(inputs, gain, forget_weight, value_weight, lower_bound[None], extra_decay)

    msgs = lax.all_to_all(
        jnp.broadcast_to(msg[None], (sp,) + msg.shape), "sp", split_axis=0, concat_axis=0,
        tiled=True,
    )
    window = jnp.left_shift(2, tp_index * pool_mix.shape[0])
    place = jnp.stack([sp_index * rows, window, sp_index]).astype(jnp.int32)
    smem = pl.BlockSpec(memory_space=pltpu.SMEM)
    local, qtot, gate, y_pool = pl.pallas_call(
        local_kernel,
        grid=(steps,),
        in_specs=[
            smem, moving(tile, width), fixed(halo_rows, width), fixed(1, width),
            fixed(width, channels), fixed(width, channels), fixed(width, channels),
            fixed(*pool_mix.shape), fixed(1, channels), fixed(1, channels),
            moving(tile, channels), moving(tile, channels), moving(tile, channels),
            moving(chunks, heads, head_k, head_k), moving(chunks, 8, channels),
        ],
        out_specs=[moving(tile, channels)] * 4,
        out_shape=[
            sds((rows, channels), f32), sds((rows, channels), bf16),
            sds((rows, channels), f32), sds((rows, channels), bf16),
        ],
        scratch_shapes=[
            pltpu.VMEM((halo_rows, channels), bf16),
            pltpu.VMEM((chunk, chunk + halo_rows), bf16),
        ],
        compiler_params=limits,
        name="local_kernel",
    )(
        place, normed, halo, gain, query_weight, outgate_weight, pool_weight, pool_mix,
        pool_scale[None], recur_gain[None], key_dec, decay, value, starts, row_info,
    )
    y_recur = pl.pallas_call(
        output_kernel,
        grid=(steps,),
        in_specs=[
            smem, fixed(*msgs.shape), fixed(*init_state.shape), moving(tile, channels),
            moving(tile, channels), moving(tile, channels),
        ],
        out_specs=moving(tile, channels),
        out_shape=sds((rows, channels), bf16),
        scratch_shapes=[pltpu.VMEM((heads, head_k, head_k), bf16)],
        compiler_params=limits,
        name="output_kernel",
    )(place, msgs, init_state, local, qtot, gate)

    def whole(weight):
        bit = 1
        stacked = weight[None]
        order = [0]
        while bit < tp:
            stacked = jnp.concatenate([stacked, swapped(stacked, "tp", tp // 2 // bit)], axis=0)
            order = order + [o ^ (tp // 2 // bit) for o in order]
            bit *= 2
        return stacked, order

    w_pool, order = whole(out_pool)
    w_recur, _ = whole(out_recur)
    pool_seen = lax.all_to_all(
        y_pool.reshape(tp, rows // tp, channels), "tp", split_axis=0, concat_axis=0, tiled=True
    )
    recur_seen = lax.all_to_all(
        y_recur.reshape(tp, rows // tp, channels), "tp", split_axis=0, concat_axis=0, tiled=True
    )
    def project(seen, weights):
        total = None
        for k, offset in enumerate(order):
            piece = lax.dynamic_index_in_dim(seen, tp_index ^ offset, 0, keepdims=False)
            term = jnp.dot(piece, weights[k], preferred_element_type=f32)
            total = term if total is None else total + term
        return total

    mixed = project(pool_seen, w_pool) + project(recur_seen, w_recur)
    return mixed.astype(bf16)


def solution(mesh):
    in_specs = (
        P("sp", None), P(), P(None, "tp"), P(None, "tp"), P(None, "tp"), P(None, "tp"),
        P(None, "tp"), P("tp", None, None), P("tp"), P("tp"), P("sp", "tp"), P("tp"),
        P("tp", None, None), P("tp", None), P("tp", None),
    )
    return jax.shard_map(
        per_device, mesh=mesh, in_specs=in_specs, out_specs=P(("sp", "tp"), None),
        check_vma=False,
    )
```

```python
import functools

import jax
import jax.numpy as jnp
from jax import lax
from jax.experimental import pallas as pl
from jax.experimental.pallas import tpu as pltpu
from jax.sharding import PartitionSpec as P


norm_eps = 1e-05
halo_rows = 16
chunk = 128
msg_pad = 16
f32 = jnp.float32
bf16 = jnp.bfloat16


def dot(a, b, dims=((1,), (0,))):
    return lax.dot_general(a, b, (dims, ((), ())), preferred_element_type=f32)


def sigmoid(x):
    return 1.0 / (1.0 + jnp.exp(-x))


def lower_triangle(size):
    row = lax.broadcasted_iota(jnp.int32, (size, size), 0)
    col = lax.broadcasted_iota(jnp.int32, (size, size), 1)
    return row >= col


def fold_gain(gain_ref, weight_refs, folded):
    lanes = gain_ref.shape[1]
    for b in range(gain_ref.shape[0]):
        rows = slice(b * lanes, (b + 1) * lanes)
        column = jnp.broadcast_to(gain_ref[b : b + 1, :], (lanes, lanes)).T
        at = 0
        for ref in weight_refs:
            for j in range(0, ref.shape[1], lanes):
                part = ref[rows, j : j + lanes].astype(f32) * column
                folded[rows, at : at + lanes] = part.astype(bf16)
                at += lanes


def row_scale(x):
    wide = x.astype(f32)
    return lax.rsqrt(jnp.mean(wide * wide, axis=-1, keepdims=True) + norm_eps)


def split(x):
    high = x.astype(bf16)
    return high, (x - high.astype(f32)).astype(bf16)


def stage_rows(stage, first, value):
    quarter = stage.shape[1]
    slot = (first // quarter) ^ lax.axis_index("tp")
    at = pl.multiple_of(first % quarter, chunk)
    stage[slot, pl.ds(at, value.shape[0]), :] = value


def unstage(stage, refs):
    @pl.when(pl.program_id(0) == pl.num_programs(0) - 1)
    def _():
        for k, ref in enumerate(refs):
            ref[...] = stage[k]


def state_kernel(
    x_ref, gain_ref, fw_ref, vw_ref, lb_ref, extra_ref,
    scale_ref, key_ref, decay_ref, value_ref, start_ref, rows_ref, msg_ref,
    folded, state, total,
):
    step = pl.program_id(0)
    heads, head_k = state.shape[0], state.shape[1]
    tile = x_ref.shape[0]
    channels = fw_ref.shape[1]

    @pl.when(step == 0)
    def _():
        state[...] = jnp.zeros_like(state)
        total[...] = jnp.zeros_like(total)
        fold_gain(gain_ref, (fw_ref, vw_ref), folded)

    x = x_ref[...]
    scale = jnp.broadcast_to(row_scale(x), scale_ref.shape)
    scale_ref[...] = scale
    raw = dot(x, folded[...])
    scales = jnp.concatenate([scale] * (channels // scale.shape[1]), axis=1)
    forget = raw[:, :channels] * scales
    value = (raw[:, channels:] * scales).astype(bf16)
    value_ref[...] = value
    gap = 1.0 - lb_ref[...]
    key = gap / (1.0 + jnp.exp(forget))
    extra_high, extra_low = split(extra_ref[...])
    pick = (
        lax.broadcasted_iota(jnp.int32, (heads, channels), 1) // head_k
        == lax.broadcasted_iota(jnp.int32, (heads, channels), 0)
    ).astype(f32).astype(bf16)
    first = ((0,), (0,))
    log_f = jnp.log(1.0 - key) + (dot(extra_high, pick, first) + dot(extra_low, pick, first))
    high, low = split(log_f)
    triangle = lower_triangle(chunk).astype(f32).astype(bf16)
    for c in range(tile // chunk):
        span = slice(c * chunk, (c + 1) * chunk)
        cum = dot(triangle, high[span]) + dot(triangle, low[span])
        middle = cum[chunk // 2 - 1 : chunk // 2]
        last = cum[chunk - 1 :]
        decay_ref[span, :] = jnp.exp(cum - middle).astype(bf16)
        key_dec = key[span] * jnp.exp(middle - cum)
        key_ref[span, :] = key_dec.astype(bf16)
        key_end = (key_dec * jnp.exp(last - middle)).astype(bf16)
        before = total[...]
        rows_ref[c] = jnp.concatenate(
            [jnp.exp(middle), jnp.exp(before), jnp.zeros((6, middle.shape[1]), f32)], axis=0
        )
        total[...] = before + last
        whole = jnp.exp(last)
        for h in range(heads):
            lanes = slice(h * head_k, (h + 1) * head_k)
            old = state[h]
            start_ref[c, h] = old.astype(bf16)
            contrib = dot(value[span, lanes], key_end[:, lanes], ((0,), (0,)))
            state[h] = old * whole[:, lanes] + contrib

    @pl.when(step == pl.num_programs(0) - 1)
    def _():
        decay_high, decay_low = split(jnp.exp(total[...]))
        for h in range(heads):
            lanes = slice(h * head_k, (h + 1) * head_k)
            ending = state[h].astype(bf16)
            decays = jnp.concatenate(
                [
                    decay_high[:, lanes].astype(f32),
                    decay_low[:, lanes].astype(f32),
                    jnp.zeros((msg_pad - 2, head_k), f32),
                ],
                axis=0,
            ).astype(bf16)
            for i in range(msg_ref.shape[0]):
                msg_ref[i, h, :head_k, :] = ending
                msg_ref[i, h, head_k:, :] = decays


def local_kernel(
    x_ref, halo_ref, gain_ref, qw_ref, ow_ref, pw_ref, mix_ref, pool_scale_ref,
    recur_gain_ref, scale_ref, key_ref, decay_ref, value_ref, start_ref, rows_ref,
    local_ref, qtot_ref, gate_ref, *rest,
):
    ypool_refs, (folded, tail, band, stage) = rest[:-4], rest[-4:]
    step = pl.program_id(0)
    tile = x_ref.shape[0]
    channels = qw_ref.shape[1]
    head_k = start_ref.shape[-1]
    heads = start_ref.shape[1]
    first_pos = lax.axis_index("sp") * (tile * pl.num_programs(0))
    window = jnp.left_shift(2, lax.axis_index("tp") * mix_ref.shape[0])

    @pl.when(step == 0)
    def _():
        fold_gain(gain_ref, (qw_ref, ow_ref, pw_ref), folded)
        halo = halo_ref[...]
        tail[...] = (dot(halo, folded[:, 2 * channels :]) * row_scale(halo)).astype(bf16)
        row = lax.broadcasted_iota(jnp.int32, band.shape, 0)
        col = lax.broadcasted_iota(jnp.int32, band.shape, 1) - halo_rows
        back = row - col
        band[...] = ((back >= 0) & (back < window)).astype(f32).astype(bf16)

    raw = dot(x_ref[...], folded[...])
    scale = scale_ref[...]
    scales = jnp.concatenate([scale] * (channels // scale.shape[1]), axis=1)
    query = raw[:, :channels] * scales
    outgate = raw[:, channels : 2 * channels] * scales
    pool_in = (raw[:, 2 * channels :] * scales).astype(bf16)
    gate_ref[...] = (outgate * sigmoid(outgate) * recur_gain_ref[...]).astype(bf16)
    query = query * sigmoid(query)
    causal = lower_triangle(chunk)
    before = tail[...]
    for c in range(tile // chunk):
        span = slice(c * chunk, (c + 1) * chunk)
        part = pool_in[span]
        sums = dot(band[...], jnp.concatenate([before, part], axis=0))
        before = part[chunk - halo_rows :]
        position = (
            first_pos + step * tile + c * chunk
            + lax.broadcasted_iota(jnp.int32, (chunk, 1), 0)
        )
        count = jnp.minimum(position + 1, window).astype(f32)
        pooled = (sums * (1.0 / count) - part.astype(f32)).astype(bf16)
        y_pool = (dot(pooled, mix_ref[0]) * pool_scale_ref[...]).astype(bf16)
        stage_rows(stage, step * tile + c * chunk, y_pool)

        query_dec = query[span] * decay_ref[span, :].astype(f32)
        query_low = query_dec.astype(bf16)
        query_abs = query_dec * rows_ref[c, 0:1, :]
        qtot_ref[span, :] = (query_abs * rows_ref[c, 1:2, :]).astype(bf16)
        query_abs = query_abs.astype(bf16)
        for h in range(heads):
            lanes = slice(h * head_k, (h + 1) * head_k)
            scores = dot(query_low[:, lanes], key_ref[span, lanes], ((1,), (1,)))
            scores = jnp.where(causal, scores, 0.0).astype(bf16)
            within = dot(scores, value_ref[span, lanes])
            earlier = dot(query_abs[:, lanes], start_ref[c, h], ((1,), (1,)))
            local_ref[span, lanes] = (within + earlier).astype(bf16)
    tail[...] = before
    unstage(stage, ypool_refs)


def output_kernel(msgs_ref, init_ref, local_ref, qtot_ref, gate_ref, *rest):
    y_refs, (carried, stage) = rest[:-2], rest[-2:]
    tile = local_ref.shape[0]
    head_k = init_ref.shape[-1]
    heads = init_ref.shape[0]

    @pl.when(pl.program_id(0) == 0)
    def _():
        for h in range(heads):
            def step(i, state):
                decay = (
                    msgs_ref[i, h, head_k : head_k + 1, :].astype(f32)
                    + msgs_ref[i, h, head_k + 1 : head_k + 2, :].astype(f32)
                )
                return state * decay + msgs_ref[i, h, :head_k, :].astype(f32)

            carried[h] = lax.fori_loop(0, lax.axis_index("sp"), step, init_ref[h].T).astype(bf16)

    pieces = []
    for h in range(heads):
        lanes = slice(h * head_k, (h + 1) * head_k)
        recur = local_ref[:, lanes].astype(f32) + dot(qtot_ref[:, lanes], carried[h], ((1,), (1,)))
        mean = jnp.mean(recur * recur, axis=-1, keepdims=True)
        scaled = recur * lax.rsqrt(mean + norm_eps)
        pieces.append((scaled * gate_ref[:, lanes].astype(f32)).astype(bf16))
    y_recur = jnp.concatenate(pieces, axis=1)
    for c in range(tile // chunk):
        rows = slice(c * chunk, (c + 1) * chunk)
        stage_rows(stage, pl.program_id(0) * tile + c * chunk, y_recur[rows])
    unstage(stage, y_refs)


def project_kernel(count, *refs):
    seen, weights, base, out_ref = refs[:count], refs[count : 2 * count], refs[2 * count : -1], refs[-1]
    total = base[0][...] if base else None
    for piece, weight in zip(seen, weights):
        term = dot(piece[...], weight[...])
        total = term if total is None else total + term
    out_ref[...] = total.astype(out_ref.dtype)


def fixed(*shape):
    return pl.BlockSpec(shape, lambda *_: (0,) * len(shape))


def moving(*shape):
    return pl.BlockSpec(shape, lambda i, *_: (i,) + (0,) * (len(shape) - 1))


limits = pltpu.CompilerParams(
    dimension_semantics=("arbitrary",), vmem_limit_bytes=56 * 1024 * 1024
)


def swapped(array, axis, bit):
    devices = lax.axis_size(axis)
    return lax.ppermute(array, axis, [(i, i ^ bit) for i in range(devices)])


def columns(size, block):
    return pl.BlockSpec((size, block), lambda i: (0, i))


def project(seen, weights, base, out_type):
    rows, channels = seen[0].shape
    width = weights[0].shape[1]
    block = min(width, 512)
    extra = [] if base is None else [base]
    return pl.pallas_call(
        functools.partial(project_kernel, len(seen)),
        grid=(width // block,),
        in_specs=[fixed(rows, channels)] * len(seen)
        + [columns(channels, block)] * len(weights)
        + [columns(rows, block)] * len(extra),
        out_specs=columns(rows, block),
        out_shape=jax.ShapeDtypeStruct((rows, width), out_type),
        compiler_params=limits,
        cost_estimate=pl.CostEstimate(
            flops=2 * len(seen) * rows * channels * width, transcendentals=0,
            bytes_accessed=2 * (len(weights) * channels * width + rows * width),
        ),
        name="project_kernel",
    )(*seen, *weights, *extra)


def per_device(
    inputs, norm_gain, pool_weight, query_weight, forget_weight, value_weight, outgate_weight,
    pool_mix, pool_scale, lower_bound, extra_decay, recur_gain, init_state, out_pool, out_recur,
):
    rows, width = inputs.shape
    heads, head_k = init_state.shape[:2]
    channels = query_weight.shape[1]
    sp, tp = lax.axis_size("sp"), lax.axis_size("tp")
    quarter, tile = rows // tp, 4 * chunk
    steps, chunks = rows // tile, tile // chunk
    lanes = 128
    gain = norm_gain.reshape(width // lanes, lanes)
    sds = jax.ShapeDtypeStruct

    def offsets_of(weight):
        far = swapped(weight, "tp", 2)
        near = swapped(weight, "tp", 1)
        return [weight, near, far, swapped(far, "tp", 1)]

    assert tp == 4
    w_pool = offsets_of(out_pool)
    w_recur = offsets_of(out_recur)

    scale, key_dec, decay, value, starts, row_info, msgs = pl.pallas_call(
        state_kernel,
        grid=(steps,),
        in_specs=[
            moving(tile, width), fixed(*gain.shape), fixed(width, channels),
            fixed(width, channels), fixed(1, channels),
            pl.BlockSpec((heads, tile), lambda i: (0, i)),
        ],
        out_specs=[
            moving(tile, lanes), moving(tile, channels), moving(tile, channels),
            moving(tile, channels), moving(chunks, heads, head_k, head_k),
            moving(chunks, 8, channels), fixed(sp, heads, head_k + msg_pad, head_k),
        ],
        out_shape=[
            sds((rows, lanes), f32), sds((rows, channels), bf16), sds((rows, channels), bf16),
            sds((rows, channels), bf16), sds((rows // chunk, heads, head_k, head_k), bf16),
            sds((rows // chunk, 8, channels), f32),
            sds((sp, heads, head_k + msg_pad, head_k), bf16),
        ],
        scratch_shapes=[
            pltpu.VMEM((width, 2 * channels), bf16), pltpu.VMEM((heads, head_k, head_k), f32),
            pltpu.VMEM((1, channels), f32),
        ],
        compiler_params=limits,
        cost_estimate=pl.CostEstimate(
            flops=4 * rows * width * channels, transcendentals=0, bytes_accessed=2 * rows * width
        ),
        name="state_kernel",
    )(inputs, gain, forget_weight, value_weight, lower_bound[None], extra_decay.T)

    halo = lax.ppermute(
        inputs[rows - halo_rows :], "sp", [(i, i + 1) for i in range(sp - 1)])
    msgs = lax.all_to_all(msgs, "sp", split_axis=0, concat_axis=0, tiled=True)
    local, qtot, gate, *y_pool = pl.pallas_call(
        local_kernel,
        grid=(steps,),
        in_specs=[
            moving(tile, width), fixed(halo_rows, width), fixed(*gain.shape),
            fixed(width, channels), fixed(width, channels), fixed(width, channels),
            fixed(*pool_mix.shape), fixed(1, channels), fixed(1, channels),
            moving(tile, lanes), moving(tile, channels), moving(tile, channels),
            moving(tile, channels), moving(chunks, heads, head_k, head_k),
            moving(chunks, 8, channels),
        ],
        out_specs=[moving(tile, channels)] * 3 + [fixed(quarter, channels)] * tp,
        out_shape=[sds((rows, channels), bf16)] * 3 + [sds((quarter, channels), bf16)] * tp,
        scratch_shapes=[
            pltpu.VMEM((width, 3 * channels), bf16),
            pltpu.VMEM((halo_rows, channels), bf16),
            pltpu.VMEM((chunk, chunk + halo_rows), bf16),
            pltpu.VMEM((tp, quarter, channels), bf16),
        ],
        compiler_params=limits,
        cost_estimate=pl.CostEstimate(
            flops=6 * rows * width * channels, transcendentals=0, bytes_accessed=2 * rows * width
        ),
        name="local_kernel",
    )(
        inputs, halo, gain, query_weight, outgate_weight, pool_weight, pool_mix,
        pool_scale[None], recur_gain[None], scale, key_dec, decay, value, starts, row_info,
    )

    def exchange(pieces):
        return [pieces[0]] + [swapped(pieces[k], "tp", k) for k in range(1, tp)]

    pool_seen = exchange(y_pool)
    out_tile = rows // 2
    y_recur = pl.pallas_call(
        output_kernel,
        grid=(rows // out_tile,),
        in_specs=[
            fixed(*msgs.shape), fixed(*init_state.shape), moving(out_tile, channels),
            moving(out_tile, channels), moving(out_tile, channels),
        ],
        out_specs=[fixed(quarter, channels)] * tp,
        out_shape=[sds((quarter, channels), bf16)] * tp,
        scratch_shapes=[
            pltpu.VMEM((heads, head_k, head_k), bf16), pltpu.VMEM((tp, quarter, channels), bf16),
        ],
        compiler_params=limits,
        cost_estimate=pl.CostEstimate(
            flops=4 * rows * head_k * channels, transcendentals=0,
            bytes_accessed=8 * rows * channels,
        ),
        name="output_kernel",
    )(msgs, init_state, local, qtot, gate)
    recur_seen = exchange(y_recur)
    partial_sum = project(pool_seen, w_pool, None, f32)
    return project(recur_seen, w_recur, partial_sum, bf16)


def solution(mesh):
    in_specs = (
        P("sp", None), P(), P(None, "tp"), P(None, "tp"), P(None, "tp"), P(None, "tp"),
        P(None, "tp"), P("tp", None, None), P("tp"), P("tp"), P("sp", "tp"), P("tp"),
        P("tp", None, None), P("tp", None), P("tp", None),
    )

    return jax.shard_map(
        per_device, mesh=mesh, in_specs=in_specs, out_specs=P(("sp", "tp"), None), check_vma=False
    )
```

```python
import functools

import jax
import jax.numpy as jnp
from jax import lax
from jax.experimental import pallas as pl
from jax.experimental.pallas import tpu as pltpu
from jax.sharding import PartitionSpec as P


norm_eps = 1e-05
halo_rows = 16
chunk = 128
msg_pad = 16
f32 = jnp.float32
bf16 = jnp.bfloat16


def dot(a, b, dims=((1,), (0,))):
    return lax.dot_general(a, b, (dims, ((), ())), preferred_element_type=f32)


def sigmoid(x):
    return 1.0 / (1.0 + jnp.exp(-x))


def lower_triangle(size):
    row = lax.broadcasted_iota(jnp.int32, (size, size), 0)
    col = lax.broadcasted_iota(jnp.int32, (size, size), 1)
    return row >= col


def fold_gain(gain_ref, weight_refs, folded):
    lanes = gain_ref.shape[1]
    for b in range(gain_ref.shape[0]):
        rows = slice(b * lanes, (b + 1) * lanes)
        column = jnp.broadcast_to(gain_ref[b : b + 1, :], (lanes, lanes)).T
        at = 0
        for ref in weight_refs:
            for j in range(0, ref.shape[1], lanes):
                part = ref[rows, j : j + lanes].astype(f32) * column
                folded[rows, at : at + lanes] = part.astype(bf16)
                at += lanes


def row_scale(x):
    wide = x.astype(f32)
    return lax.rsqrt(jnp.mean(wide * wide, axis=-1, keepdims=True) + norm_eps)


def split(x):
    high = x.astype(bf16)
    return high, (x - high.astype(f32)).astype(bf16)


def stage_rows(stage, first, value):
    quarter = stage.shape[1]
    slot = (first // quarter) ^ lax.axis_index("tp")
    at = pl.multiple_of(first % quarter, chunk)
    stage[slot, pl.ds(at, value.shape[0]), :] = value


def unstage(stage, refs):
    @pl.when(pl.program_id(0) == pl.num_programs(0) - 1)
    def _():
        for k, ref in enumerate(refs):
            ref[...] = stage[k]


def state_kernel(
    x_ref, gain_ref, fw_ref, vw_ref, lb_ref, extra_ref,
    scale_ref, key_ref, decay_ref, value_ref, start_ref, rows_ref, msg_ref,
    folded, state, total,
):
    step = pl.program_id(0)
    heads, head_k = state.shape[0], state.shape[1]
    tile = x_ref.shape[0]
    channels = fw_ref.shape[1]

    @pl.when(step == 0)
    def _():
        state[...] = jnp.zeros_like(state)
        total[...] = jnp.zeros_like(total)
        fold_gain(gain_ref, (fw_ref, vw_ref), folded)

    gap = 1.0 - lb_ref[...]
    pick = (
        lax.broadcasted_iota(jnp.int32, (heads, channels), 1) // head_k
        == lax.broadcasted_iota(jnp.int32, (heads, channels), 0)
    ).astype(f32).astype(bf16)
    triangle = lower_triangle(chunk).astype(f32).astype(bf16)
    triangle = jnp.concatenate([triangle, triangle], axis=1)
    first = ((0,), (0,))

    def project_block(b):
        return dot(x_ref[b * 256 : (b + 1) * 256, :], folded[...])

    extra_high, extra_low = split(extra_ref[...])
    extras = dot(extra_high, pick, first) + dot(extra_low, pick, first)
    ahead = project_block(0)
    scale_ref[...] = jnp.broadcast_to(row_scale(x_ref[...]), scale_ref.shape)
    for b in range(tile // 256):
        block = slice(b * 256, (b + 1) * 256)
        raw = ahead
        if (b + 1) * 256 < tile:
            ahead = project_block(b + 1)
        scale = scale_ref[block, :]
        scales = jnp.concatenate([scale] * (channels // scale.shape[1]), axis=1)
        forget = raw[:, :channels] * scales
        value = (raw[:, channels:] * scales).astype(bf16)
        value_ref[block, :] = value
        key = gap / (1.0 + jnp.exp(forget))
        extra = extras[block]
        high, low = split(jnp.log(1.0 - key) + extra)
        for j in range(256 // chunk):
            c = b * (256 // chunk) + j
            part = slice(j * chunk, (j + 1) * chunk)
            span = slice(c * chunk, (c + 1) * chunk)
            cum = dot(triangle, jnp.concatenate([high[part], low[part]], axis=0))
            middle = cum[chunk // 2 - 1 : chunk // 2]
            last = cum[chunk - 1 :]
            decay_ref[span, :] = jnp.exp(cum - middle).astype(bf16)
            key_dec = key[part] * jnp.exp(middle - cum)
            key_ref[span, :] = key_dec.astype(bf16)
            key_end = (key_dec * jnp.exp(last - middle)).astype(bf16)
            before = total[...]
            rows_ref[c] = jnp.concatenate(
                [jnp.exp(middle), jnp.exp(before), jnp.zeros((6, middle.shape[1]), f32)], axis=0
            )
            total[...] = before + last
            whole = jnp.exp(last)
            for h in range(heads):
                lanes = slice(h * head_k, (h + 1) * head_k)
                old = state[h]
                start_ref[c, h] = old.astype(bf16)
                contrib = dot(value[part, lanes], key_end[:, lanes], first)
                state[h] = old * whole[:, lanes] + contrib

    @pl.when(step == pl.num_programs(0) - 1)
    def _():
        decay_high, decay_low = split(jnp.exp(total[...]))
        for h in range(heads):
            lanes = slice(h * head_k, (h + 1) * head_k)
            ending = state[h].astype(bf16)
            decays = jnp.concatenate(
                [
                    decay_high[:, lanes].astype(f32),
                    decay_low[:, lanes].astype(f32),
                    jnp.zeros((msg_pad - 2, head_k), f32),
                ],
                axis=0,
            ).astype(bf16)
            for i in range(msg_ref.shape[0]):
                msg_ref[i, h, :head_k, :] = ending
                msg_ref[i, h, head_k:, :] = decays


def local_kernel(
    x_ref, halo_ref, gain_ref, qw_ref, ow_ref, pw_ref, mix_ref, pool_scale_ref,
    recur_gain_ref, scale_ref, key_ref, decay_ref, value_ref, start_ref, rows_ref,
    local_ref, qtot_ref, gate_ref, *rest,
):
    ypool_refs, (folded, tail, band, stage) = rest[:-4], rest[-4:]
    step = pl.program_id(0)
    tile = x_ref.shape[0]
    channels = qw_ref.shape[1]
    head_k = start_ref.shape[-1]
    heads = start_ref.shape[1]
    first_pos = lax.axis_index("sp") * (tile * pl.num_programs(0))
    window = jnp.left_shift(2, lax.axis_index("tp") * mix_ref.shape[0])

    @pl.when(step == 0)
    def _():
        fold_gain(gain_ref, (qw_ref, ow_ref, pw_ref), folded)
        halo = halo_ref[...]
        tail[...] = (dot(halo, folded[:, 2 * channels :]) * row_scale(halo)).astype(bf16)
        row = lax.broadcasted_iota(jnp.int32, band.shape, 0)
        col = lax.broadcasted_iota(jnp.int32, band.shape, 1) - halo_rows
        back = row - col
        band[...] = ((back >= 0) & (back < window)).astype(f32).astype(bf16)

    causal = lower_triangle(chunk)
    before = tail[...]

    def project_block(b):
        return dot(x_ref[b * 256 : (b + 1) * 256, :], folded[...])

    ahead = project_block(0)
    for b in range(tile // 256):
        block = slice(b * 256, (b + 1) * 256)
        raw = ahead
        if (b + 1) * 256 < tile:
            ahead = project_block(b + 1)
        scale = scale_ref[block, :]
        scales = jnp.concatenate([scale] * (channels // scale.shape[1]), axis=1)
        query = raw[:, :channels] * scales
        outgate = raw[:, channels : 2 * channels] * scales
        pool_in = (raw[:, 2 * channels :] * scales).astype(bf16)
        gate_ref[block, :] = (outgate * sigmoid(outgate) * recur_gain_ref[...]).astype(bf16)
        query = query * sigmoid(query)
        for j in range(256 // chunk):
            c = b * (256 // chunk) + j
            part = slice(j * chunk, (j + 1) * chunk)
            span = slice(c * chunk, (c + 1) * chunk)
            pool_part = pool_in[part]
            sums = dot(band[...], jnp.concatenate([before, pool_part], axis=0))
            before = pool_part[chunk - halo_rows :]
            position = (
                first_pos + step * tile + c * chunk
                + lax.broadcasted_iota(jnp.int32, (chunk, 1), 0)
            )
            count = jnp.minimum(position + 1, window).astype(f32)
            pooled = (sums * (1.0 / count) - pool_part.astype(f32)).astype(bf16)
            y_pool = (dot(pooled, mix_ref[0]) * pool_scale_ref[...]).astype(bf16)
            stage_rows(stage, step * tile + c * chunk, y_pool)

            query_dec = query[part] * decay_ref[span, :].astype(f32)
            query_low = query_dec.astype(bf16)
            query_abs = query_dec * rows_ref[c, 0:1, :]
            qtot_ref[span, :] = (query_abs * rows_ref[c, 1:2, :]).astype(bf16)
            query_abs = query_abs.astype(bf16)
            for h in range(heads):
                lanes = slice(h * head_k, (h + 1) * head_k)
                scores = dot(query_low[:, lanes], key_ref[span, lanes], ((1,), (1,)))
                scores = jnp.where(causal, scores, 0.0).astype(bf16)
                within = dot(scores, value_ref[span, lanes])
                earlier = dot(query_abs[:, lanes], start_ref[c, h], ((1,), (1,)))
                local_ref[span, lanes] = (within + earlier).astype(bf16)
    tail[...] = before
    unstage(stage, ypool_refs)


def output_kernel(msgs_ref, init_ref, local_ref, qtot_ref, gate_ref, *rest):
    y_refs, (carried, stage) = rest[:-2], rest[-2:]
    tile = local_ref.shape[0]
    head_k = init_ref.shape[-1]
    heads = init_ref.shape[0]

    @pl.when(pl.program_id(0) == 0)
    def _():
        for h in range(heads):
            def step(i, state):
                decay = (
                    msgs_ref[i, h, head_k : head_k + 1, :].astype(f32)
                    + msgs_ref[i, h, head_k + 1 : head_k + 2, :].astype(f32)
                )
                return state * decay + msgs_ref[i, h, :head_k, :].astype(f32)

            carried[h] = lax.fori_loop(0, lax.axis_index("sp"), step, init_ref[h].T).astype(bf16)

    pieces = []
    for h in range(heads):
        lanes = slice(h * head_k, (h + 1) * head_k)
        recur = local_ref[:, lanes].astype(f32) + dot(qtot_ref[:, lanes], carried[h], ((1,), (1,)))
        mean = jnp.mean(recur * recur, axis=-1, keepdims=True)
        scaled = recur * lax.rsqrt(mean + norm_eps)
        pieces.append((scaled * gate_ref[:, lanes].astype(f32)).astype(bf16))
    y_recur = jnp.concatenate(pieces, axis=1)
    for c in range(tile // chunk):
        rows = slice(c * chunk, (c + 1) * chunk)
        stage_rows(stage, pl.program_id(0) * tile + c * chunk, y_recur[rows])
    unstage(stage, y_refs)


def project_kernel(counts, *refs):
    refs = list(refs)
    seen = [refs.pop(0) for _ in counts]
    groups = [[refs.pop(0) for _ in range(count)] for count in counts]
    out_ref = refs.pop()
    total = refs.pop()[...].astype(f32) if refs else None
    second = pl.program_id(0) >= pl.num_programs(0) // 2
    for piece, group in zip(seen, groups):
        weight = group[0][...]
        if len(group) > 1:
            mine = (lax.axis_index("sp") % 2 == 1) == second
            weight = jnp.where(mine, weight, group[1][...])
        term = dot(piece[...], weight)
        total = term if total is None else total + term
    out_ref[...] = total.astype(out_ref.dtype)


def fixed(*shape):
    return pl.BlockSpec(shape, lambda *_: (0,) * len(shape))


def moving(*shape):
    return pl.BlockSpec(shape, lambda i, *_: (i,) + (0,) * (len(shape) - 1))


def limits(mib):
    return pltpu.CompilerParams(
        dimension_semantics=("arbitrary",), vmem_limit_bytes=mib * 1024 * 1024
    )


def swapped(array, axis, bit):
    devices = lax.axis_size(axis)
    return lax.ppermute(array, axis, [(i, i ^ bit) for i in range(devices)])


def columns(size, block):
    return pl.BlockSpec((size, block), lambda i: (0, i))


def half_columns(size, width, block, mine):
    count = width // block // 2

    def index(i):
        parity = lax.axis_index("sp") % 2
        half = parity if mine else 1 - parity
        return 0, jnp.clip(i - count * half, 0, count - 1)

    return pl.BlockSpec((size, block), index)


def project(seen, weights, base, out_type):
    rows, channels = seen[0].shape
    width = weights[0][0].shape[1] * len(weights[0])
    block = width // 4
    extra = [] if base is None else [base]
    flat = [array for group in weights for array in group]
    counts = tuple(len(group) for group in weights)
    specs = []
    for count in counts:
        if count == 1:
            specs.append(columns(channels, block))
        else:
            specs += [half_columns(channels, width, block, mine) for mine in (True, False)]
    return pl.pallas_call(
        functools.partial(project_kernel, counts),
        grid=(width // block,),
        in_specs=[fixed(rows, channels)] * len(seen) + specs
        + [columns(rows, block)] * len(extra),
        out_specs=columns(rows, block),
        out_shape=jax.ShapeDtypeStruct((rows, width), out_type),
        compiler_params=limits(32),
        cost_estimate=pl.CostEstimate(
            flops=2 * len(seen) * rows * channels * width, transcendentals=0,
            bytes_accessed=2 * (len(weights) * channels * width + rows * width),
        ),
        name="project_kernel",
    )(*seen, *flat, *extra)


def per_device(
    inputs, norm_gain, pool_weight, query_weight, forget_weight, value_weight, outgate_weight,
    pool_mix, pool_scale, lower_bound, extra_decay, recur_gain, init_state, out_pool, out_recur,
):
    rows, width = inputs.shape
    heads, head_k = init_state.shape[:2]
    channels = query_weight.shape[1]
    sp, tp = lax.axis_size("sp"), lax.axis_size("tp")
    quarter, tile = rows // tp, 4 * chunk
    steps, chunks = rows // tile, tile // chunk
    lanes = 128
    gain = norm_gain.reshape(width // lanes, lanes)
    sds = jax.ShapeDtypeStruct

    assert tp == 4 and sp % 2 == 0
    far = swapped(out_pool, "tp", 2)
    half_width = width // 2
    half = lax.dynamic_slice_in_dim(
        out_recur, (lax.axis_index("sp") % 2) * half_width, half_width, axis=1
    )
    fetched = swapped(half, "tp", 2)
    handed = swapped(fetched, "sp", 1)
    cross_fetched = swapped(fetched, "tp", 1)
    cross_handed = swapped(handed, "tp", 1)
    w_pool = [
        [out_pool], [swapped(out_pool, "tp", 1)], [far],
        [swapped(far, "tp", 1)],
    ]
    w_recur = [
        [out_recur], [swapped(out_recur, "tp", 1)], [fetched, handed],
        [cross_fetched, cross_handed],
    ]

    scale, key_dec, decay, value, starts, row_info, msgs = pl.pallas_call(
        state_kernel,
        grid=(steps,),
        in_specs=[
            moving(tile, width), fixed(*gain.shape), fixed(width, channels),
            fixed(width, channels), fixed(1, channels),
            pl.BlockSpec((heads, tile), lambda i: (0, i)),
        ],
        out_specs=[
            moving(tile, lanes), moving(tile, channels), moving(tile, channels),
            moving(tile, channels), moving(chunks, heads, head_k, head_k),
            moving(chunks, 8, channels), fixed(sp, heads, head_k + msg_pad, head_k),
        ],
        out_shape=[
            sds((rows, lanes), f32), sds((rows, channels), bf16), sds((rows, channels), bf16),
            sds((rows, channels), bf16), sds((rows // chunk, heads, head_k, head_k), bf16),
            sds((rows // chunk, 8, channels), f32),
            sds((sp, heads, head_k + msg_pad, head_k), bf16),
        ],
        scratch_shapes=[
            pltpu.VMEM((width, 2 * channels), bf16), pltpu.VMEM((heads, head_k, head_k), f32),
            pltpu.VMEM((1, channels), f32),
        ],
        compiler_params=limits(60),
        cost_estimate=pl.CostEstimate(
            flops=4 * rows * width * channels, transcendentals=0, bytes_accessed=2 * rows * width
        ),
        name="state_kernel",
    )(inputs, gain, forget_weight, value_weight, lower_bound[None], extra_decay.T)

    halo = lax.ppermute(
        inputs[rows - halo_rows :], "sp", [(i, i + 1) for i in range(sp - 1)])
    msgs = lax.all_to_all(msgs, "sp", split_axis=0, concat_axis=0, tiled=True)
    local, qtot, gate, *y_pool = pl.pallas_call(
        local_kernel,
        grid=(steps,),
        in_specs=[
            moving(tile, width), fixed(halo_rows, width), fixed(*gain.shape),
            fixed(width, channels), fixed(width, channels), fixed(width, channels),
            fixed(*pool_mix.shape), fixed(1, channels), fixed(1, channels),
            moving(tile, lanes), moving(tile, channels), moving(tile, channels),
            moving(tile, channels), moving(chunks, heads, head_k, head_k),
            moving(chunks, 8, channels),
        ],
        out_specs=[moving(tile, channels)] * 3 + [fixed(quarter, channels)] * tp,
        out_shape=[sds((rows, channels), bf16)] * 3 + [sds((quarter, channels), bf16)] * tp,
        scratch_shapes=[
            pltpu.VMEM((width, 3 * channels), bf16),
            pltpu.VMEM((halo_rows, channels), bf16),
            pltpu.VMEM((chunk, chunk + halo_rows), bf16),
            pltpu.VMEM((tp, quarter, channels), bf16),
        ],
        compiler_params=limits(54),
        cost_estimate=pl.CostEstimate(
            flops=6 * rows * width * channels, transcendentals=0, bytes_accessed=2 * rows * width
        ),
        name="local_kernel",
    )(
        inputs, halo, gain, query_weight, outgate_weight, pool_weight, pool_mix,
        pool_scale[None], recur_gain[None], scale, key_dec, decay, value, starts, row_info,
    )

    def exchange(pieces):
        return [pieces[0]] + [swapped(pieces[k], "tp", k) for k in range(1, tp)]

    pool_seen = exchange(y_pool)
    out_tile = rows // 2
    y_recur = pl.pallas_call(
        output_kernel,
        grid=(rows // out_tile,),
        in_specs=[
            fixed(*msgs.shape), fixed(*init_state.shape), moving(out_tile, channels),
            moving(out_tile, channels), moving(out_tile, channels),
        ],
        out_specs=[fixed(quarter, channels)] * tp,
        out_shape=[sds((quarter, channels), bf16)] * tp,
        scratch_shapes=[
            pltpu.VMEM((heads, head_k, head_k), bf16), pltpu.VMEM((tp, quarter, channels), bf16),
        ],
        compiler_params=limits(40),
        cost_estimate=pl.CostEstimate(
            flops=4 * rows * head_k * channels, transcendentals=0,
            bytes_accessed=8 * rows * channels,
        ),
        name="output_kernel",
    )(msgs, init_state, local, qtot, gate)
    recur_seen = exchange(y_recur)
    partial_sum = project(pool_seen + recur_seen[:2], w_pool + w_recur[:2], None, bf16)
    return project(recur_seen[2:], w_recur[2:], partial_sum, bf16)


def solution(mesh):
    in_specs = (
        P("sp", None), P(), P(None, "tp"), P(None, "tp"), P(None, "tp"), P(None, "tp"),
        P(None, "tp"), P("tp", None, None), P("tp"), P("tp"), P("sp", "tp"), P("tp"),
        P("tp", None, None), P("tp", None), P("tp", None),
    )

    return jax.shard_map(
        per_device, mesh=mesh, in_specs=in_specs, out_specs=P(("sp", "tp"), None), check_vma=False
    )
```

```python
import functools

import jax
import jax.numpy as jnp
from jax import lax
from jax.experimental import pallas as pl
from jax.experimental.pallas import tpu as pltpu
from jax.sharding import PartitionSpec as P


norm_eps = 1e-05
halo_rows = 16
chunk = 128
msg_pad = 16
f32 = jnp.float32
bf16 = jnp.bfloat16


def dot(a, b, dims=((1,), (0,))):
    return lax.dot_general(a, b, (dims, ((), ())), preferred_element_type=f32)


def sigmoid(x):
    return 1.0 / (1.0 + jnp.exp(-x))


def lower_triangle(size):
    row = lax.broadcasted_iota(jnp.int32, (size, size), 0)
    col = lax.broadcasted_iota(jnp.int32, (size, size), 1)
    return row >= col


def fold_gain(gain_ref, weight_refs, folded):
    lanes = gain_ref.shape[1]
    for b in range(gain_ref.shape[0]):
        rows = slice(b * lanes, (b + 1) * lanes)
        column = jnp.broadcast_to(gain_ref[b : b + 1, :], (lanes, lanes)).T
        at = 0
        for ref in weight_refs:
            for j in range(0, ref.shape[1], lanes):
                part = ref[rows, j : j + lanes].astype(f32) * column
                folded[rows, at : at + lanes] = part.astype(bf16)
                at += lanes


def row_scale(x):
    wide = x.astype(f32)
    return lax.rsqrt(jnp.mean(wide * wide, axis=-1, keepdims=True) + norm_eps)


def split(x):
    high = x.astype(bf16)
    return high, (x - high.astype(f32)).astype(bf16)


def stage_rows(stage, first, value):
    quarter = stage.shape[1]
    slot = (first // quarter) ^ lax.axis_index("tp")
    at = pl.multiple_of(first % quarter, chunk)
    stage[slot, pl.ds(at, value.shape[0]), :] = value


def unstage(stage, refs):
    @pl.when(pl.program_id(0) == pl.num_programs(0) - 1)
    def _():
        for k, ref in enumerate(refs):
            ref[...] = stage[k]


def state_kernel(
    x_ref, halo_ref, gain_ref, fw_ref, vw_ref, pw_ref, mix_ref, pool_scale_ref, lb_ref,
    extra_ref, weight_ref, scale_ref, kept_ref, start_ref, rows_ref, msg_ref, half_ref, *rest,
):
    ypool_refs, (folded, state, total, tail, band, stage) = rest[:-6], rest[-6:]
    step = pl.program_id(0)
    first_pos = lax.axis_index("sp") * (x_ref.shape[0] * pl.num_programs(0))
    window = jnp.left_shift(2, lax.axis_index("tp") * mix_ref.shape[0])
    heads, head_k = state.shape[0], state.shape[1]
    tile = x_ref.shape[0]
    channels = fw_ref.shape[1]

    @pl.when(step == 0)
    def _():
        state[...] = jnp.zeros_like(state)
        total[...] = jnp.zeros_like(total)
        half_ref[...] = weight_ref[...]
        fold_gain(gain_ref, (fw_ref, vw_ref, pw_ref), folded)
        halo = halo_ref[...]
        tail[...] = (dot(halo, folded[:, 2 * channels :]) * row_scale(halo)).astype(bf16)
        row = lax.broadcasted_iota(jnp.int32, band.shape, 0)
        col = lax.broadcasted_iota(jnp.int32, band.shape, 1) - halo_rows
        back = row - col
        band[...] = ((back >= 0) & (back < window)).astype(f32).astype(bf16)

    gap = 1.0 - lb_ref[...]
    pick = (
        lax.broadcasted_iota(jnp.int32, (heads, channels), 1) // head_k
        == lax.broadcasted_iota(jnp.int32, (heads, channels), 0)
    ).astype(f32).astype(bf16)
    triangle = lower_triangle(chunk).astype(f32).astype(bf16)
    triangle = jnp.concatenate([triangle, triangle], axis=1)
    first = ((0,), (0,))

    def project_block(b):
        return dot(x_ref[b * 256 : (b + 1) * 256, :], folded[...])

    extra_high, extra_low = split(extra_ref[...])
    extras = dot(extra_high, pick, first) + dot(extra_low, pick, first)
    tail_rows = tail[...]
    ahead = project_block(0)
    scale_ref[...] = jnp.broadcast_to(row_scale(x_ref[...]), scale_ref.shape)
    for b in range(tile // 256):
        block = slice(b * 256, (b + 1) * 256)
        raw = ahead
        if (b + 1) * 256 < tile:
            ahead = project_block(b + 1)
        scale = scale_ref[block, :]
        scales = jnp.concatenate([scale] * (channels // scale.shape[1]), axis=1)
        forget = raw[:, :channels] * scales
        value = (raw[:, channels : 2 * channels] * scales).astype(bf16)
        kept_ref[block, 2 * channels :] = value
        pool_in = (raw[:, 2 * channels :] * scales).astype(bf16)
        key = gap / (1.0 + jnp.exp(forget))
        extra = extras[block]
        high, low = split(jnp.log(1.0 - key) + extra)
        for j in range(256 // chunk):
            c = b * (256 // chunk) + j
            part = slice(j * chunk, (j + 1) * chunk)
            span = slice(c * chunk, (c + 1) * chunk)
            cum = dot(triangle, jnp.concatenate([high[part], low[part]], axis=0))
            middle = cum[chunk // 2 - 1 : chunk // 2]
            last = cum[chunk - 1 :]
            kept_ref[span, channels : 2 * channels] = jnp.exp(cum - middle).astype(bf16)
            key_dec = key[part] * jnp.exp(middle - cum)
            kept_ref[span, :channels] = key_dec.astype(bf16)
            key_end = (key_dec * jnp.exp(last - middle)).astype(bf16)
            before = total[...]
            rows_ref[c] = jnp.concatenate(
                [jnp.exp(middle), jnp.exp(before), jnp.zeros((6, middle.shape[1]), f32)], axis=0
            )
            total[...] = before + last
            whole = jnp.exp(last)
            for h in range(heads):
                lanes = slice(h * head_k, (h + 1) * head_k)
                old = state[h]
                start_ref[c, h] = old.astype(bf16)
                contrib = dot(value[part, lanes], key_end[:, lanes], first)
                state[h] = old * whole[:, lanes] + contrib

            pool_part = pool_in[part]
            sums = dot(band[...], jnp.concatenate([tail_rows, pool_part], axis=0))
            tail_rows = pool_part[chunk - halo_rows :]
            position = (
                first_pos + step * tile + c * chunk
                + lax.broadcasted_iota(jnp.int32, (chunk, 1), 0)
            )
            count = jnp.minimum(position + 1, window).astype(f32)
            pooled = (sums * (1.0 / count) - pool_part.astype(f32)).astype(bf16)
            y_pool = (dot(pooled, mix_ref[0]) * pool_scale_ref[...]).astype(bf16)
            stage_rows(stage, step * tile + c * chunk, y_pool)
    tail[...] = tail_rows
    unstage(stage, ypool_refs)

    @pl.when(step == pl.num_programs(0) - 1)
    def _():
        decay_high, decay_low = split(jnp.exp(total[...]))
        for h in range(heads):
            lanes = slice(h * head_k, (h + 1) * head_k)
            ending = state[h].astype(bf16)
            decays = jnp.concatenate(
                [
                    decay_high[:, lanes].astype(f32),
                    decay_low[:, lanes].astype(f32),
                    jnp.zeros((msg_pad - 2, head_k), f32),
                ],
                axis=0,
            ).astype(bf16)
            for i in range(msg_ref.shape[0]):
                msg_ref[i, h, :head_k, :] = ending
                msg_ref[i, h, head_k:, :] = decays


def local_kernel(
    x_ref, gain_ref, qw_ref, ow_ref, recur_gain_ref, scale_ref, kept_ref, start_ref, rows_ref,
    parts_ref, folded,
):
    step = pl.program_id(0)
    tile = x_ref.shape[0]
    channels = qw_ref.shape[1]
    head_k = start_ref.shape[-1]
    heads = start_ref.shape[1]

    @pl.when(step == 0)
    def _():
        fold_gain(gain_ref, (qw_ref, ow_ref), folded)

    causal = lower_triangle(chunk)

    def project_block(b):
        return dot(x_ref[b * 256 : (b + 1) * 256, :], folded[...])

    ahead = project_block(0)
    for b in range(tile // 256):
        block = slice(b * 256, (b + 1) * 256)
        raw = ahead
        if (b + 1) * 256 < tile:
            ahead = project_block(b + 1)
        scale = scale_ref[block, :]
        scales = jnp.concatenate([scale] * (channels // scale.shape[1]), axis=1)
        query = raw[:, :channels] * scales
        outgate = raw[:, channels:] * scales
        gate = outgate * sigmoid(outgate) * recur_gain_ref[...]
        parts_ref[block, 2 * channels :] = gate.astype(bf16)
        query = query * sigmoid(query)
        for j in range(256 // chunk):
            c = b * (256 // chunk) + j
            part = slice(j * chunk, (j + 1) * chunk)
            span = slice(c * chunk, (c + 1) * chunk)
            query_dec = query[part] * kept_ref[span, channels : 2 * channels].astype(f32)
            query_low = query_dec.astype(bf16)
            query_abs = query_dec * rows_ref[c, 0:1, :]
            parts_ref[span, channels : 2 * channels] = (query_abs * rows_ref[c, 1:2, :]).astype(bf16)
            query_abs = query_abs.astype(bf16)
            for h in range(heads):
                lanes = slice(h * head_k, (h + 1) * head_k)
                key = kept_ref[span, lanes]
                value = kept_ref[span, 2 * channels + h * head_k : 2 * channels + (h + 1) * head_k]
                scores = dot(query_low[:, lanes], key, ((1,), (1,)))
                scores = jnp.where(causal, scores, 0.0).astype(bf16)
                within = dot(scores, value)
                earlier = dot(query_abs[:, lanes], start_ref[c, h], ((1,), (1,)))
                parts_ref[span, lanes] = (within + earlier).astype(bf16)


def output_kernel(msgs_ref, init_ref, parts_ref, *rest):
    y_refs, carried = rest[:-1], rest[-1]
    channels = parts_ref.shape[1] // 3
    head_k = init_ref.shape[-1]
    heads = init_ref.shape[0]

    @pl.when(pl.program_id(0) == 0)
    def _():
        for h in range(heads):
            def step(i, state):
                decay = (
                    msgs_ref[i, h, head_k : head_k + 1, :].astype(f32)
                    + msgs_ref[i, h, head_k + 1 : head_k + 2, :].astype(f32)
                )
                return state * decay + msgs_ref[i, h, :head_k, :].astype(f32)

            carried[h] = lax.fori_loop(0, lax.axis_index("sp"), step, init_ref[h].T).astype(bf16)

    pieces = []
    for h in range(heads):
        local, qtot, gate = [
            parts_ref[:, k * channels + h * head_k : k * channels + (h + 1) * head_k]
            for k in range(3)
        ]
        recur = local.astype(f32) + dot(qtot, carried[h], ((1,), (1,)))
        mean = jnp.mean(recur * recur, axis=-1, keepdims=True)
        scaled = recur * lax.rsqrt(mean + norm_eps)
        pieces.append((scaled * gate.astype(f32)).astype(bf16))
    y_recur = jnp.concatenate(pieces, axis=1)
    for k, ref in enumerate(y_refs):
        @pl.when(pl.program_id(0) == k)
        def _():
            ref[...] = y_recur


def project_kernel(counts, *refs):
    refs = list(refs)
    seen = [refs.pop(0) for _ in counts]
    groups = [[refs.pop(0) for _ in range(count)] for count in counts]
    out_ref = refs.pop()
    total = refs.pop()[...].astype(f32) if refs else None
    for piece, group in zip(seen, groups):
        weight = group[0][...]
        if len(group) > 1:
            other, even = group[1][...], lax.axis_index("sp") % 2 == 0
            weight = jnp.concatenate(
                [jnp.where(even, weight, other), jnp.where(even, other, weight)], axis=0
            )
        term = dot(piece[...], weight)
        total = term if total is None else total + term
    out_ref[...] = total.astype(out_ref.dtype)


def fixed(*shape):
    return pl.BlockSpec(shape, lambda *_: (0,) * len(shape))


def moving(*shape):
    return pl.BlockSpec(shape, lambda i, *_: (i,) + (0,) * (len(shape) - 1))


def limits(mib):
    return pltpu.CompilerParams(
        dimension_semantics=("arbitrary",), vmem_limit_bytes=mib * 1024 * 1024
    )


def swapped(array, axis, bit):
    devices = lax.axis_size(axis)
    return lax.ppermute(array, axis, [(i, i ^ bit) for i in range(devices)])


def columns(size, block):
    return pl.BlockSpec((size, block), lambda i: (0, i))


def project(seen, weights, base, out_type):
    rows, channels = seen[0].shape
    width = weights[0][0].shape[1]
    block = width // 2
    extra = [] if base is None else [base]
    flat = [array for group in weights for array in group]
    counts = tuple(len(group) for group in weights)
    specs = [columns(channels // count, block) for count in counts for _ in range(count)]
    return pl.pallas_call(
        functools.partial(project_kernel, counts),
        grid=(width // block,),
        in_specs=[fixed(rows, channels)] * len(seen) + specs
        + [columns(rows, block)] * len(extra),
        out_specs=columns(rows, block),
        out_shape=jax.ShapeDtypeStruct((rows, width), out_type),
        compiler_params=limits(32),
        cost_estimate=pl.CostEstimate(
            flops=2 * len(seen) * rows * channels * width, transcendentals=0,
            bytes_accessed=2 * (len(weights) * channels * width + rows * width),
        ),
        name="project_kernel",
    )(*seen, *flat, *extra)


def per_device(
    inputs, norm_gain, pool_weight, query_weight, forget_weight, value_weight, outgate_weight,
    pool_mix, pool_scale, lower_bound, extra_decay, recur_gain, init_state, out_pool, out_recur,
):
    rows, width = inputs.shape
    heads, head_k = init_state.shape[:2]
    channels = query_weight.shape[1]
    sp, tp = lax.axis_size("sp"), lax.axis_size("tp")
    quarter, tile = rows // tp, 4 * chunk
    steps, chunks = rows // tile, tile // chunk
    lanes = 128
    gain = norm_gain.reshape(width // lanes, lanes)
    sds = jax.ShapeDtypeStruct

    assert tp == 4 and sp % 2 == 0
    far = swapped(out_pool, "tp", 2)
    w_pool = [
        [out_pool], [swapped(out_pool, "tp", 1)], [far],
        [swapped(far, "tp", 1)],
    ]
    halo = lax.ppermute(inputs[rows - halo_rows :], "sp", [(i, i + 1) for i in range(sp - 1)])
    scale, kept, starts, row_info, msgs, half, *y_pool = pl.pallas_call(
        state_kernel,
        grid=(steps,),
        in_specs=[
            moving(tile, width), fixed(halo_rows, width), fixed(*gain.shape),
            fixed(width, channels), fixed(width, channels), fixed(width, channels),
            fixed(*pool_mix.shape), fixed(1, channels), fixed(1, channels),
            pl.BlockSpec((heads, tile), lambda i: (0, i)),
            pl.BlockSpec((channels // 2, width), lambda i: (lax.axis_index("sp") % 2, 0)),
        ],
        out_specs=[
            moving(tile, lanes), moving(tile, 3 * channels),
            moving(chunks, heads, head_k, head_k), moving(chunks, 8, channels),
            fixed(sp, heads, head_k + msg_pad, head_k), fixed(channels // 2, width),
        ] + [fixed(quarter, channels)] * tp,
        out_shape=[
            sds((rows, lanes), f32), sds((rows, 3 * channels), bf16),
            sds((rows // chunk, heads, head_k, head_k), bf16),
            sds((rows // chunk, 8, channels), f32),
            sds((sp, heads, head_k + msg_pad, head_k), bf16), sds((channels // 2, width), bf16),
        ] + [sds((quarter, channels), bf16)] * tp,
        scratch_shapes=[
            pltpu.VMEM((width, 3 * channels), bf16), pltpu.VMEM((heads, head_k, head_k), f32),
            pltpu.VMEM((1, channels), f32), pltpu.VMEM((halo_rows, channels), bf16),
            pltpu.VMEM((chunk, chunk + halo_rows), bf16),
            pltpu.VMEM((tp, quarter, channels), bf16),
        ],
        compiler_params=limits(58),
        cost_estimate=pl.CostEstimate(
            flops=6 * rows * width * channels, transcendentals=0, bytes_accessed=2 * rows * width
        ),
        name="state_kernel",
    )(
        inputs, halo, gain, forget_weight, value_weight, pool_weight, pool_mix, pool_scale[None],
        lower_bound[None], extra_decay.T, out_recur,
    )
    fetched = swapped(half, "tp", 2)
    handed = swapped(fetched, "sp", 1)
    cross_fetched = swapped(fetched, "tp", 1)
    cross_handed = swapped(handed, "tp", 1)
    w_recur = [
        [out_recur], [swapped(out_recur, "tp", 1)], [fetched, handed],
        [cross_fetched, cross_handed],
    ]


    def exchange(pieces):
        return [pieces[0]] + [swapped(pieces[k], "tp", k) for k in range(1, tp)]

    msgs = lax.all_to_all(msgs, "sp", split_axis=0, concat_axis=0, tiled=True)
    pool_seen = exchange(y_pool)
    parts = pl.pallas_call(
        local_kernel,
        grid=(steps,),
        in_specs=[
            moving(tile, width), fixed(*gain.shape), fixed(width, channels),
            fixed(width, channels), fixed(1, channels),
            moving(tile, lanes), moving(tile, 3 * channels),
            moving(chunks, heads, head_k, head_k), moving(chunks, 8, channels),
        ],
        out_specs=moving(tile, 3 * channels),
        out_shape=sds((rows, 3 * channels), bf16),
        scratch_shapes=[pltpu.VMEM((width, 2 * channels), bf16)],
        compiler_params=limits(54),
        cost_estimate=pl.CostEstimate(
            flops=4 * rows * width * channels, transcendentals=0, bytes_accessed=2 * rows * width
        ),
        name="local_kernel",
    )(
        inputs, gain, query_weight, outgate_weight, recur_gain[None], scale, kept, starts, row_info,
    )

    def outputs(flip):
        part = pl.BlockSpec(
            (quarter, 3 * channels), lambda i: (lax.axis_index("tp") ^ (flip + i), 0)
        )
        return pl.pallas_call(
            output_kernel,
            grid=(2,),
            in_specs=[fixed(*msgs.shape), fixed(*init_state.shape), part],
            out_specs=[fixed(quarter, channels)] * 2,
            out_shape=[sds((quarter, channels), bf16)] * 2,
            scratch_shapes=[pltpu.VMEM((heads, head_k, head_k), bf16)],
            compiler_params=limits(40),
            cost_estimate=pl.CostEstimate(
                flops=2 * rows * head_k * channels, transcendentals=0,
                bytes_accessed=4 * rows * channels,
            ),
            name="output_kernel",
        )(msgs, init_state, parts)

    far_y = outputs(2)
    near_y = outputs(0)
    y_recur = near_y + far_y
    recur_seen = exchange(y_recur)
    partial_sum = project(pool_seen + recur_seen[:2], w_pool + w_recur[:2], None, bf16)
    return project(recur_seen[2:], w_recur[2:], partial_sum, bf16)


def solution(mesh):
    in_specs = (
        P("sp", None), P(), P(None, "tp"), P(None, "tp"), P(None, "tp"), P(None, "tp"),
        P(None, "tp"), P("tp", None, None), P("tp"), P("tp"), P("sp", "tp"), P("tp"),
        P("tp", None, None), P("tp", None), P("tp", None),
    )

    return jax.shard_map(
        per_device, mesh=mesh, in_specs=in_specs, out_specs=P(("sp", "tp"), None), check_vma=False
    )
```

```python
import functools

import jax
import jax.numpy as jnp
from jax import lax
from jax.experimental import pallas as pl
from jax.experimental.pallas import tpu as pltpu
from jax.sharding import PartitionSpec as P


norm_eps = 1e-05
halo_rows = 16
chunk = 128
msg_pad = 16
f32 = jnp.float32
bf16 = jnp.bfloat16


def dot(a, b, dims=((1,), (0,))):
    return lax.dot_general(a, b, (dims, ((), ())), preferred_element_type=f32)


def sigmoid(x):
    return 1.0 / (1.0 + jnp.exp(-x))


def lower_triangle(size):
    row = lax.broadcasted_iota(jnp.int32, (size, size), 0)
    col = lax.broadcasted_iota(jnp.int32, (size, size), 1)
    return row >= col


def fold_gain(gain_ref, weight_refs, folded):
    lanes = gain_ref.shape[1]
    for b in range(gain_ref.shape[0]):
        rows = slice(b * lanes, (b + 1) * lanes)
        column = jnp.broadcast_to(gain_ref[b : b + 1, :], (lanes, lanes)).T
        at = 0
        for ref in weight_refs:
            for j in range(0, ref.shape[1], lanes):
                part = ref[rows, j : j + lanes].astype(f32) * column
                folded[rows, at : at + lanes] = part.astype(bf16)
                at += lanes


def row_scale(x):
    wide = x.astype(f32)
    return lax.rsqrt(jnp.mean(wide * wide, axis=-1, keepdims=True) + norm_eps)


def split(x):
    high = x.astype(bf16)
    return high, (x - high.astype(f32)).astype(bf16)


def stage_rows(stage, first, value):
    quarter = stage.shape[1]
    slot = (first // quarter) ^ lax.axis_index("tp")
    at = pl.multiple_of(first % quarter, chunk)
    stage[slot, pl.ds(at, value.shape[0]), :] = value


def unstage(stage, refs):
    @pl.when(pl.program_id(0) == pl.num_programs(0) - 1)
    def _():
        for k, ref in enumerate(refs):
            ref[...] = stage[k]


def state_kernel(
    x_ref, halo_ref, gain_ref, fw_ref, vw_ref, pw_ref, mix_ref, pool_scale_ref, lb_ref,
    extra_ref, scale_ref, kept_ref, start_ref, rows_ref, msg_ref, *rest,
):
    ypool_refs, (folded, state, total, tail, band, stage) = rest[:-6], rest[-6:]
    step = pl.program_id(0)
    first_pos = lax.axis_index("sp") * (x_ref.shape[0] * pl.num_programs(0))
    window = jnp.left_shift(2, lax.axis_index("tp") * mix_ref.shape[0])
    heads, head_k = state.shape[0], state.shape[1]
    tile = x_ref.shape[0]
    channels = fw_ref.shape[1]

    @pl.when(step == 0)
    def _():
        state[...] = jnp.zeros_like(state)
        total[...] = jnp.zeros_like(total)
        fold_gain(gain_ref, (fw_ref, vw_ref, pw_ref), folded)
        halo = halo_ref[...]
        tail[...] = (dot(halo, folded[:, 2 * channels :]) * row_scale(halo)).astype(bf16)
        row = lax.broadcasted_iota(jnp.int32, band.shape, 0)
        col = lax.broadcasted_iota(jnp.int32, band.shape, 1) - halo_rows
        back = row - col
        band[...] = ((back >= 0) & (back < window)).astype(f32).astype(bf16)

    gap = 1.0 - lb_ref[...]
    pick = (
        lax.broadcasted_iota(jnp.int32, (heads, channels), 1) // head_k
        == lax.broadcasted_iota(jnp.int32, (heads, channels), 0)
    ).astype(f32).astype(bf16)
    triangle = lower_triangle(chunk).astype(f32).astype(bf16)
    triangle = jnp.concatenate([triangle, triangle], axis=1)
    first = ((0,), (0,))

    def project_block(b):
        return dot(x_ref[b * 256 : (b + 1) * 256, :], folded[...])

    extra_high, extra_low = split(extra_ref[...])
    extras = dot(extra_high, pick, first) + dot(extra_low, pick, first)
    tail_rows = tail[...]
    ahead = project_block(0)
    scale_ref[...] = jnp.broadcast_to(row_scale(x_ref[...]), scale_ref.shape)
    for b in range(tile // 256):
        block = slice(b * 256, (b + 1) * 256)
        raw = ahead
        if (b + 1) * 256 < tile:
            ahead = project_block(b + 1)
        scale = scale_ref[block, :]
        scales = jnp.concatenate([scale] * (channels // scale.shape[1]), axis=1)
        forget = raw[:, :channels] * scales
        value = (raw[:, channels : 2 * channels] * scales).astype(bf16)
        kept_ref[block, 2 * channels :] = value
        pool_in = (raw[:, 2 * channels :] * scales).astype(bf16)
        key = gap / (1.0 + jnp.exp(forget))
        extra = extras[block]
        high, low = split(jnp.log(1.0 - key) + extra)
        for j in range(256 // chunk):
            c = b * (256 // chunk) + j
            part = slice(j * chunk, (j + 1) * chunk)
            span = slice(c * chunk, (c + 1) * chunk)
            cum = dot(triangle, jnp.concatenate([high[part], low[part]], axis=0))
            middle = cum[chunk // 2 - 1 : chunk // 2]
            last = cum[chunk - 1 :]
            kept_ref[span, channels : 2 * channels] = jnp.exp(cum - middle).astype(bf16)
            key_dec = key[part] * jnp.exp(middle - cum)
            kept_ref[span, :channels] = key_dec.astype(bf16)
            key_end = (key_dec * jnp.exp(last - middle)).astype(bf16)
            before = total[...]
            rows_ref[c] = jnp.concatenate(
                [jnp.exp(middle), jnp.exp(before), jnp.zeros((6, middle.shape[1]), f32)], axis=0
            )
            total[...] = before + last
            whole = jnp.exp(last)
            for h in range(heads):
                lanes = slice(h * head_k, (h + 1) * head_k)
                old = state[h]
                start_ref[c, h] = old.astype(bf16)
                contrib = dot(value[part, lanes], key_end[:, lanes], first)
                state[h] = old * whole[:, lanes] + contrib

            pool_part = pool_in[part]
            sums = dot(band[...], jnp.concatenate([tail_rows, pool_part], axis=0))
            tail_rows = pool_part[chunk - halo_rows :]
            position = (
                first_pos + step * tile + c * chunk
                + lax.broadcasted_iota(jnp.int32, (chunk, 1), 0)
            )
            count = jnp.minimum(position + 1, window).astype(f32)
            pooled = (sums * (1.0 / count) - pool_part.astype(f32)).astype(bf16)
            y_pool = (dot(pooled, mix_ref[0]) * pool_scale_ref[...]).astype(bf16)
            stage_rows(stage, step * tile + c * chunk, y_pool)
    tail[...] = tail_rows
    unstage(stage, ypool_refs)

    @pl.when(step == pl.num_programs(0) - 1)
    def _():
        decay_high, decay_low = split(jnp.exp(total[...]))
        for h in range(heads):
            lanes = slice(h * head_k, (h + 1) * head_k)
            ending = state[h].astype(bf16)
            decays = jnp.concatenate(
                [
                    decay_high[:, lanes].astype(f32),
                    decay_low[:, lanes].astype(f32),
                    jnp.zeros((msg_pad - 2, head_k), f32),
                ],
                axis=0,
            ).astype(bf16)
            for i in range(msg_ref.shape[0]):
                msg_ref[i, h, :head_k, :] = ending
                msg_ref[i, h, head_k:, :] = decays


def local_kernel(
    x_ref, gain_ref, qw_ref, ow_ref, recur_gain_ref, scale_ref, kept_ref, start_ref, rows_ref,
    parts_ref, folded, diagonal,
):
    step = pl.program_id(0)
    tile = x_ref.shape[0]
    channels = qw_ref.shape[1]
    head_k = start_ref.shape[-1]
    heads = start_ref.shape[1]

    @pl.when(step == 0)
    def _():
        fold_gain(gain_ref, (qw_ref, ow_ref), folded)
        diagonal[...] = jnp.zeros_like(diagonal)

    causal = jnp.concatenate([lower_triangle(chunk)] * heads, axis=1)

    def project_block(b):
        return dot(x_ref[b * 256 : (b + 1) * 256, :], folded[...])

    ahead = project_block(0)
    for b in range(tile // 256):
        block = slice(b * 256, (b + 1) * 256)
        raw = ahead
        if (b + 1) * 256 < tile:
            ahead = project_block(b + 1)
        scale = scale_ref[block, :]
        scales = jnp.concatenate([scale] * (channels // scale.shape[1]), axis=1)
        query = raw[:, :channels] * scales
        outgate = raw[:, channels:] * scales
        gate = outgate * sigmoid(outgate) * recur_gain_ref[...]
        parts_ref[block, 2 * channels :] = gate.astype(bf16)
        query = query * sigmoid(query)
        for j in range(256 // chunk):
            c = b * (256 // chunk) + j
            part = slice(j * chunk, (j + 1) * chunk)
            span = slice(c * chunk, (c + 1) * chunk)
            query_dec = query[part] * kept_ref[span, channels : 2 * channels].astype(f32)
            query_low = query_dec.astype(bf16)
            query_abs = query_dec * rows_ref[c, 0:1, :]
            parts_ref[span, channels : 2 * channels] = (query_abs * rows_ref[c, 1:2, :]).astype(bf16)
            query_abs = query_abs.astype(bf16)
            keys, values, states = [diagonal.at[3 * (c % 2) + k] for k in range(3)]
            for h in range(heads):
                lanes = slice(h * head_k, (h + 1) * head_k)
                keys[lanes, lanes] = kept_ref[span, lanes]
                values[lanes, lanes] = kept_ref[
                    span, 2 * channels + h * head_k : 2 * channels + (h + 1) * head_k
                ]
                states[lanes, lanes] = start_ref[c, h]
            scores = dot(query_low, keys[...], ((1,), (1,)))
            scores = jnp.where(causal, scores, 0.0).astype(bf16)
            within = dot(scores, values[...])
            earlier = dot(query_abs, states[...], ((1,), (1,)))
            parts_ref[span, :channels] = (within + earlier).astype(bf16)


def output_kernel(msgs_ref, init_ref, parts_ref, *rest):
    y_refs, carried = rest[:-1], rest[-1]
    channels = parts_ref.shape[1] // 3
    head_k = init_ref.shape[-1]
    heads = init_ref.shape[0]

    @pl.when(pl.program_id(0) == 0)
    def _():
        for h in range(heads):
            def step(i, state):
                decay = (
                    msgs_ref[i, h, head_k : head_k + 1, :].astype(f32)
                    + msgs_ref[i, h, head_k + 1 : head_k + 2, :].astype(f32)
                )
                return state * decay + msgs_ref[i, h, :head_k, :].astype(f32)

            carried[h] = lax.fori_loop(0, lax.axis_index("sp"), step, init_ref[h].T).astype(bf16)

    pieces = []
    for h in range(heads):
        local, qtot, gate = [
            parts_ref[:, k * channels + h * head_k : k * channels + (h + 1) * head_k]
            for k in range(3)
        ]
        recur = local.astype(f32) + dot(qtot, carried[h], ((1,), (1,)))
        mean = jnp.mean(recur * recur, axis=-1, keepdims=True)
        scaled = recur * lax.rsqrt(mean + norm_eps)
        pieces.append((scaled * gate.astype(f32)).astype(bf16))
    y_recur = jnp.concatenate(pieces, axis=1)
    for k, ref in enumerate(y_refs):
        @pl.when(pl.program_id(0) == k)
        def _():
            ref[...] = y_recur


def project_kernel(counts, *refs):
    refs = list(refs)
    seen = [refs.pop(0) for _ in counts]
    groups = [[refs.pop(0) for _ in range(count)] for count in counts]
    out_ref = refs.pop()
    total = refs.pop()[...].astype(f32) if refs else None
    for piece, group in zip(seen, groups):
        weight = group[0][...]
        if len(group) > 1:
            other, even = group[1][...], lax.axis_index("sp") % 2 == 0
            weight = jnp.concatenate(
                [jnp.where(even, weight, other), jnp.where(even, other, weight)], axis=0
            )
        term = dot(piece[...], weight)
        total = term if total is None else total + term
    out_ref[...] = total.astype(out_ref.dtype)


def fixed(*shape):
    return pl.BlockSpec(shape, lambda *_: (0,) * len(shape))


def moving(*shape):
    return pl.BlockSpec(shape, lambda i, *_: (i,) + (0,) * (len(shape) - 1))


def limits(mib):
    return pltpu.CompilerParams(
        dimension_semantics=("arbitrary",), vmem_limit_bytes=mib * 1024 * 1024
    )


def swapped(array, axis, bit):
    devices = lax.axis_size(axis)
    return lax.ppermute(array, axis, [(i, i ^ bit) for i in range(devices)])


def columns(size, block):
    return pl.BlockSpec((size, block), lambda i: (0, i))


def project(seen, weights, base, out_type):
    rows, channels = seen[0].shape
    width = weights[0][0].shape[1]
    block = width // 2
    extra = [] if base is None else [base]
    flat = [array for group in weights for array in group]
    counts = tuple(len(group) for group in weights)
    specs = [columns(channels // count, block) for count in counts for _ in range(count)]
    return pl.pallas_call(
        functools.partial(project_kernel, counts),
        grid=(width // block,),
        in_specs=[fixed(rows, channels)] * len(seen) + specs
        + [columns(rows, block)] * len(extra),
        out_specs=columns(rows, block),
        out_shape=jax.ShapeDtypeStruct((rows, width), out_type),
        compiler_params=limits(32),
        cost_estimate=pl.CostEstimate(
            flops=2 * len(seen) * rows * channels * width, transcendentals=0,
            bytes_accessed=2 * (len(weights) * channels * width + rows * width),
        ),
        name="project_kernel",
    )(*seen, *flat, *extra)


def per_device(
    inputs, norm_gain, pool_weight, query_weight, forget_weight, value_weight, outgate_weight,
    pool_mix, pool_scale, lower_bound, extra_decay, recur_gain, init_state, out_pool, out_recur,
):
    rows, width = inputs.shape
    heads, head_k = init_state.shape[:2]
    channels = query_weight.shape[1]
    sp, tp = lax.axis_size("sp"), lax.axis_size("tp")
    quarter, tile = rows // tp, 4 * chunk
    steps, chunks = rows // tile, tile // chunk
    lanes = 128
    gain = norm_gain.reshape(width // lanes, lanes)
    sds = jax.ShapeDtypeStruct

    assert tp == 4 and sp % 2 == 0
    far = swapped(out_pool, "tp", 2)
    w_pool = [
        [out_pool], [swapped(out_pool, "tp", 1)], [far],
        [swapped(far, "tp", 1)],
    ]
    halo = lax.ppermute(inputs[rows - halo_rows :], "sp", [(i, i + 1) for i in range(sp - 1)])
    scale, kept, starts, row_info, msgs, *y_pool = pl.pallas_call(
        state_kernel,
        grid=(steps,),
        in_specs=[
            moving(tile, width), fixed(halo_rows, width), fixed(*gain.shape),
            fixed(width, channels), fixed(width, channels), fixed(width, channels),
            fixed(*pool_mix.shape), fixed(1, channels), fixed(1, channels),
            pl.BlockSpec((heads, tile), lambda i: (0, i)),
        ],
        out_specs=[
            moving(tile, lanes), moving(tile, 3 * channels),
            moving(chunks, heads, head_k, head_k), moving(chunks, 8, channels),
            fixed(sp, heads, head_k + msg_pad, head_k),
        ] + [fixed(quarter, channels)] * tp,
        out_shape=[
            sds((rows, lanes), f32), sds((rows, 3 * channels), bf16),
            sds((rows // chunk, heads, head_k, head_k), bf16),
            sds((rows // chunk, 8, channels), f32),
            sds((sp, heads, head_k + msg_pad, head_k), bf16),
        ] + [sds((quarter, channels), bf16)] * tp,
        scratch_shapes=[
            pltpu.VMEM((width, 3 * channels), bf16), pltpu.VMEM((heads, head_k, head_k), f32),
            pltpu.VMEM((1, channels), f32), pltpu.VMEM((halo_rows, channels), bf16),
            pltpu.VMEM((chunk, chunk + halo_rows), bf16),
            pltpu.VMEM((tp, quarter, channels), bf16),
        ],
        compiler_params=limits(58),
        cost_estimate=pl.CostEstimate(
            flops=6 * rows * width * channels, transcendentals=0, bytes_accessed=2 * rows * width
        ),
        name="state_kernel",
    )(
        inputs, halo, gain, forget_weight, value_weight, pool_weight, pool_mix, pool_scale[None],
        lower_bound[None], extra_decay.T,
    )
    half = lax.dynamic_slice_in_dim(
        out_recur, (lax.axis_index("sp") % 2) * (channels // 2), channels // 2, axis=0
    )
    fetched = swapped(half, "tp", 2)
    handed = swapped(fetched, "sp", 1)
    cross_fetched = swapped(fetched, "tp", 1)
    cross_handed = swapped(handed, "tp", 1)
    w_recur = [
        [out_recur], [swapped(out_recur, "tp", 1)], [fetched, handed],
        [cross_fetched, cross_handed],
    ]


    def exchange(pieces):
        return [pieces[0]] + [swapped(pieces[k], "tp", k) for k in range(1, tp)]

    msgs = lax.all_to_all(msgs, "sp", split_axis=0, concat_axis=0, tiled=True)
    pool_seen = exchange(y_pool)
    parts = pl.pallas_call(
        local_kernel,
        grid=(steps,),
        in_specs=[
            moving(tile, width), fixed(*gain.shape), fixed(width, channels),
            fixed(width, channels), fixed(1, channels),
            moving(tile, lanes), moving(tile, 3 * channels),
            moving(chunks, heads, head_k, head_k), moving(chunks, 8, channels),
        ],
        out_specs=moving(tile, 3 * channels),
        out_shape=sds((rows, 3 * channels), bf16),
        scratch_shapes=[
            pltpu.VMEM((width, 2 * channels), bf16), pltpu.VMEM((6, channels, channels), bf16),
        ],
        compiler_params=limits(54),
        cost_estimate=pl.CostEstimate(
            flops=4 * rows * width * channels, transcendentals=0, bytes_accessed=2 * rows * width
        ),
        name="local_kernel",
    )(
        inputs, gain, query_weight, outgate_weight, recur_gain[None], scale, kept, starts, row_info,
    )

    def outputs(flip):
        part = pl.BlockSpec(
            (quarter, 3 * channels), lambda i: (lax.axis_index("tp") ^ (flip + i), 0)
        )
        return pl.pallas_call(
            output_kernel,
            grid=(2,),
            in_specs=[fixed(*msgs.shape), fixed(*init_state.shape), part],
            out_specs=[fixed(quarter, channels)] * 2,
            out_shape=[sds((quarter, channels), bf16)] * 2,
            scratch_shapes=[pltpu.VMEM((heads, head_k, head_k), bf16)],
            compiler_params=limits(40),
            cost_estimate=pl.CostEstimate(
                flops=2 * rows * head_k * channels, transcendentals=0,
                bytes_accessed=4 * rows * channels,
            ),
            name="output_kernel",
        )(msgs, init_state, parts)

    far_y = outputs(2)
    near_y = outputs(0)
    y_recur = near_y + far_y
    recur_seen = exchange(y_recur)
    partial_sum = project(pool_seen + recur_seen[:2], w_pool + w_recur[:2], None, bf16)
    return project(recur_seen[2:], w_recur[2:], partial_sum, bf16)


def solution(mesh):
    in_specs = (
        P("sp", None), P(), P(None, "tp"), P(None, "tp"), P(None, "tp"), P(None, "tp"),
        P(None, "tp"), P("tp", None, None), P("tp"), P("tp"), P("sp", "tp"), P("tp"),
        P("tp", None, None), P("tp", None), P("tp", None),
    )

    return jax.shard_map(
        per_device, mesh=mesh, in_specs=in_specs, out_specs=P(("sp", "tp"), None), check_vma=False
    )
```

```python
import functools

import jax
import jax.numpy as jnp
from jax import lax
from jax.experimental import pallas as pl
from jax.experimental.pallas import tpu as pltpu
from jax.sharding import PartitionSpec as P


norm_eps = 1e-05
halo_rows = 16
chunk = 128
msg_pad = 16
f32 = jnp.float32
bf16 = jnp.bfloat16


def dot(a, b, dims=((1,), (0,))):
    return lax.dot_general(a, b, (dims, ((), ())), preferred_element_type=f32)


def sigmoid(x):
    return 1.0 / (1.0 + jnp.exp(-x))


def lower_triangle(size):
    row = lax.broadcasted_iota(jnp.int32, (size, size), 0)
    col = lax.broadcasted_iota(jnp.int32, (size, size), 1)
    return row >= col


def fold_gain(gain_ref, weight_refs, folded):
    lanes = gain_ref.shape[1]
    for b in range(gain_ref.shape[0]):
        rows = slice(b * lanes, (b + 1) * lanes)
        column = jnp.broadcast_to(gain_ref[b : b + 1, :], (lanes, lanes)).T
        at = 0
        for ref in weight_refs:
            for j in range(0, ref.shape[1], lanes):
                part = ref[rows, j : j + lanes].astype(f32) * column
                folded[rows, at : at + lanes] = part.astype(bf16)
                at += lanes


def row_scale(x):
    wide = x.astype(f32)
    return lax.rsqrt(jnp.mean(wide * wide, axis=-1, keepdims=True) + norm_eps)


def split(x):
    high = x.astype(bf16)
    return high, (x - high.astype(f32)).astype(bf16)


def stage_rows(stage, first, value):
    quarter = stage.shape[1]
    slot = (first // quarter) ^ lax.axis_index("tp")
    at = pl.multiple_of(first % quarter, chunk)
    stage[slot, pl.ds(at, value.shape[0]), :] = value


def unstage(stage, refs):
    @pl.when(pl.program_id(0) == pl.num_programs(0) - 1)
    def _():
        for k, ref in enumerate(refs):
            ref[...] = stage[k]


def state_kernel(
    x_ref, halo_ref, gain_ref, fw_ref, vw_ref, pw_ref, mix_ref, pool_scale_ref, lb_ref,
    extra_ref, scale_ref, kept_ref, start_ref, rows_ref, msg_ref, *rest,
):
    ypool_refs, (folded, state, total, tail, band, stage) = rest[:-6], rest[-6:]
    step = pl.program_id(0)
    first_pos = lax.axis_index("sp") * (x_ref.shape[0] * pl.num_programs(0))
    window = jnp.left_shift(2, lax.axis_index("tp") * mix_ref.shape[0])
    heads, head_k = state.shape[0], state.shape[1]
    tile = x_ref.shape[0]
    channels = fw_ref.shape[1]

    @pl.when(step == 0)
    def _():
        state[...] = jnp.zeros_like(state)
        total[...] = jnp.zeros_like(total)
        fold_gain(gain_ref, (fw_ref, vw_ref, pw_ref), folded)
        halo = halo_ref[...]
        tail[...] = (dot(halo, folded[:, 2 * channels :]) * row_scale(halo)).astype(bf16)
        row = lax.broadcasted_iota(jnp.int32, band.shape, 0)
        col = lax.broadcasted_iota(jnp.int32, band.shape, 1) - halo_rows
        back = row - col
        band[...] = ((back >= 0) & (back < window)).astype(f32).astype(bf16)

    gap = 1.0 - lb_ref[...]
    pick = (
        lax.broadcasted_iota(jnp.int32, (heads, channels), 1) // head_k
        == lax.broadcasted_iota(jnp.int32, (heads, channels), 0)
    ).astype(f32).astype(bf16)
    triangle = lower_triangle(chunk).astype(f32).astype(bf16)
    triangle = jnp.concatenate([triangle, triangle], axis=1)
    first = ((0,), (0,))

    def project_block(b):
        return dot(x_ref[b * 256 : (b + 1) * 256, :], folded[...])

    extra_high, extra_low = split(extra_ref[...])
    extras = dot(extra_high, pick, first) + dot(extra_low, pick, first)
    tail_rows = tail[...]
    ahead = project_block(0)
    scale_ref[...] = jnp.broadcast_to(row_scale(x_ref[...]), scale_ref.shape)
    for b in range(tile // 256):
        block = slice(b * 256, (b + 1) * 256)
        raw = ahead
        if (b + 1) * 256 < tile:
            ahead = project_block(b + 1)
        scale = scale_ref[block, :]
        scales = jnp.concatenate([scale] * (channels // scale.shape[1]), axis=1)
        forget = raw[:, :channels] * scales
        value = (raw[:, channels : 2 * channels] * scales).astype(bf16)
        kept_ref[block, 2 * channels :] = value
        pool_in = (raw[:, 2 * channels :] * scales).astype(bf16)
        key = gap / (1.0 + jnp.exp(forget))
        extra = extras[block]
        high, low = split(jnp.log(1.0 - key) + extra)
        for j in range(256 // chunk):
            c = b * (256 // chunk) + j
            part = slice(j * chunk, (j + 1) * chunk)
            span = slice(c * chunk, (c + 1) * chunk)
            cum = dot(triangle, jnp.concatenate([high[part], low[part]], axis=0))
            middle = cum[chunk // 2 - 1 : chunk // 2]
            last = cum[chunk - 1 :]
            kept_ref[span, channels : 2 * channels] = jnp.exp(cum - middle).astype(bf16)
            key_dec = key[part] * jnp.exp(middle - cum)
            kept_ref[span, :channels] = key_dec.astype(bf16)
            key_end = (key_dec * jnp.exp(last - middle)).astype(bf16)
            before = total[...]
            rows_ref[c] = jnp.concatenate(
                [jnp.exp(middle), jnp.exp(before), jnp.zeros((6, middle.shape[1]), f32)], axis=0
            )
            total[...] = before + last
            whole = jnp.exp(last)
            for h in range(heads):
                lanes = slice(h * head_k, (h + 1) * head_k)
                old = state[h]
                start_ref[c, h] = old.astype(bf16)
                contrib = dot(value[part, lanes], key_end[:, lanes], first)
                state[h] = old * whole[:, lanes] + contrib

            pool_part = pool_in[part]
            sums = dot(band[...], jnp.concatenate([tail_rows, pool_part], axis=0))
            tail_rows = pool_part[chunk - halo_rows :]
            position = (
                first_pos + step * tile + c * chunk
                + lax.broadcasted_iota(jnp.int32, (chunk, 1), 0)
            )
            count = jnp.minimum(position + 1, window).astype(f32)
            pooled = (sums * (1.0 / count) - pool_part.astype(f32)).astype(bf16)
            y_pool = (dot(pooled, mix_ref[0]) * pool_scale_ref[...]).astype(bf16)
            stage_rows(stage, step * tile + c * chunk, y_pool)
    tail[...] = tail_rows
    unstage(stage, ypool_refs)

    @pl.when(step == pl.num_programs(0) - 1)
    def _():
        decay_high, decay_low = split(jnp.exp(total[...]))
        decays = [
            part[:, h * head_k : (h + 1) * head_k].astype(f32)
            for h in range(heads) for part in (decay_high, decay_low)
        ]
        decays.append(jnp.zeros((msg_pad - 2 * heads, head_k), f32))
        decays = jnp.concatenate(decays, axis=0).astype(bf16)
        endings = [state[h].astype(bf16) for h in range(heads)]
        for i in range(msg_ref.shape[0]):
            for h in range(heads):
                msg_ref[i, h * head_k : (h + 1) * head_k, :] = endings[h]
            msg_ref[i, heads * head_k :, :] = decays


def local_kernel(
    x_ref, gain_ref, qw_ref, ow_ref, recur_gain_ref, scale_ref, kept_ref, start_ref, rows_ref,
    parts_ref, folded, diagonal,
):
    step = pl.program_id(0)
    tile = x_ref.shape[0]
    channels = qw_ref.shape[1]
    head_k = start_ref.shape[-1]
    heads = start_ref.shape[1]

    @pl.when(step == 0)
    def _():
        fold_gain(gain_ref, (qw_ref, ow_ref), folded)
        diagonal[...] = jnp.zeros_like(diagonal)

    causal = jnp.concatenate([lower_triangle(chunk)] * heads, axis=1)

    def project_block(b):
        return dot(x_ref[b * 256 : (b + 1) * 256, :], folded[...])

    ahead = project_block(0)
    for b in range(tile // 256):
        block = slice(b * 256, (b + 1) * 256)
        raw = ahead
        if (b + 1) * 256 < tile:
            ahead = project_block(b + 1)
        scale = scale_ref[block, :]
        scales = jnp.concatenate([scale] * (channels // scale.shape[1]), axis=1)
        query = raw[:, :channels] * scales
        outgate = raw[:, channels:] * scales
        gate = outgate * sigmoid(outgate) * recur_gain_ref[...]
        parts_ref[block, 2 * channels :] = gate.astype(bf16)
        query = query * sigmoid(query)
        for j in range(256 // chunk):
            c = b * (256 // chunk) + j
            part = slice(j * chunk, (j + 1) * chunk)
            span = slice(c * chunk, (c + 1) * chunk)
            query_dec = query[part] * kept_ref[span, channels : 2 * channels].astype(f32)
            query_low = query_dec.astype(bf16)
            query_abs = query_dec * rows_ref[c, 0:1, :]
            parts_ref[span, channels : 2 * channels] = (query_abs * rows_ref[c, 1:2, :]).astype(bf16)
            query_abs = query_abs.astype(bf16)
            keys, values, states = [diagonal.at[3 * (c % 2) + k] for k in range(3)]
            for h in range(heads):
                lanes = slice(h * head_k, (h + 1) * head_k)
                keys[lanes, lanes] = kept_ref[span, lanes]
                values[lanes, lanes] = kept_ref[
                    span, 2 * channels + h * head_k : 2 * channels + (h + 1) * head_k
                ]
                states[lanes, lanes] = start_ref[c, h]
            scores = dot(query_low, keys[...], ((1,), (1,)))
            scores = jnp.where(causal, scores, 0.0).astype(bf16)
            within = dot(scores, values[...])
            earlier = dot(query_abs, states[...], ((1,), (1,)))
            parts_ref[span, :channels] = (within + earlier).astype(bf16)


def output_kernel(msgs_ref, init_ref, parts_ref, *rest):
    y_refs, carried = rest[:-1], rest[-1]
    channels = parts_ref.shape[1] // 3
    head_k = init_ref.shape[-1]
    heads = init_ref.shape[0]

    @pl.when(pl.program_id(0) == 0)
    def _():
        for h in range(heads):
            def step(i, state):
                at = heads * head_k + 2 * h
                decay = (
                    msgs_ref[i, at : at + 1, :].astype(f32)
                    + msgs_ref[i, at + 1 : at + 2, :].astype(f32)
                )
                return state * decay + msgs_ref[i, h * head_k : (h + 1) * head_k, :].astype(f32)

            carried[h] = lax.fori_loop(0, lax.axis_index("sp"), step, init_ref[h].T).astype(bf16)

    pieces = []
    for h in range(heads):
        local, qtot, gate = [
            parts_ref[:, k * channels + h * head_k : k * channels + (h + 1) * head_k]
            for k in range(3)
        ]
        recur = local.astype(f32) + dot(qtot, carried[h], ((1,), (1,)))
        mean = jnp.mean(recur * recur, axis=-1, keepdims=True)
        scaled = recur * lax.rsqrt(mean + norm_eps)
        pieces.append((scaled * gate.astype(f32)).astype(bf16))
    y_recur = jnp.concatenate(pieces, axis=1)
    for k, ref in enumerate(y_refs):
        @pl.when(pl.program_id(0) == k)
        def _():
            ref[...] = y_recur


def project_kernel(counts, *refs):
    refs = list(refs)
    seen = [refs.pop(0) for _ in counts]
    groups = [[refs.pop(0) for _ in range(count)] for count in counts]
    out_ref = refs.pop()
    total = refs.pop()[...].astype(f32) if refs else None
    for piece, group in zip(seen, groups):
        weight = group[0][...]
        if len(group) > 1:
            other, even = group[1][...], lax.axis_index("sp") % 2 == 0
            weight = jnp.concatenate(
                [jnp.where(even, weight, other), jnp.where(even, other, weight)], axis=0
            )
        term = dot(piece[...], weight)
        total = term if total is None else total + term
    out_ref[...] = total.astype(out_ref.dtype)


def fixed(*shape):
    return pl.BlockSpec(shape, lambda *_: (0,) * len(shape))


def moving(*shape):
    return pl.BlockSpec(shape, lambda i, *_: (i,) + (0,) * (len(shape) - 1))


def limits(mib):
    return pltpu.CompilerParams(
        dimension_semantics=("arbitrary",), vmem_limit_bytes=mib * 1024 * 1024
    )


def swapped(array, axis, bit):
    devices = lax.axis_size(axis)
    return lax.ppermute(array, axis, [(i, i ^ bit) for i in range(devices)])


def columns(size, block):
    return pl.BlockSpec((size, block), lambda i: (0, i))


def project(seen, weights, base, out_type):
    rows, channels = seen[0].shape
    width = weights[0][0].shape[1]
    block = width // 2
    extra = [] if base is None else [base]
    flat = [array for group in weights for array in group]
    counts = tuple(len(group) for group in weights)
    specs = [columns(channels // count, block) for count in counts for _ in range(count)]
    return pl.pallas_call(
        functools.partial(project_kernel, counts),
        grid=(width // block,),
        in_specs=[fixed(rows, channels)] * len(seen) + specs
        + [columns(rows, block)] * len(extra),
        out_specs=columns(rows, block),
        out_shape=jax.ShapeDtypeStruct((rows, width), out_type),
        compiler_params=limits(32),
        cost_estimate=pl.CostEstimate(
            flops=2 * len(seen) * rows * channels * width, transcendentals=0,
            bytes_accessed=2 * (len(weights) * channels * width + rows * width),
        ),
        name="project_kernel",
    )(*seen, *flat, *extra)


def per_device(
    inputs, norm_gain, pool_weight, query_weight, forget_weight, value_weight, outgate_weight,
    pool_mix, pool_scale, lower_bound, extra_decay, recur_gain, init_state, out_pool, out_recur,
):
    rows, width = inputs.shape
    heads, head_k = init_state.shape[:2]
    channels = query_weight.shape[1]
    sp, tp = lax.axis_size("sp"), lax.axis_size("tp")
    quarter, tile = rows // tp, 4 * chunk
    steps, chunks = rows // tile, tile // chunk
    lanes = 128
    gain = norm_gain.reshape(width // lanes, lanes)
    sds = jax.ShapeDtypeStruct

    assert tp == 4 and sp % 2 == 0
    far = swapped(out_pool, "tp", 2)
    w_pool = [
        [out_pool], [swapped(out_pool, "tp", 1)], [far],
        [swapped(far, "tp", 1)],
    ]
    halo = lax.ppermute(inputs[rows - halo_rows :], "sp", [(i, i + 1) for i in range(sp - 1)])
    scale, kept, starts, row_info, msgs, *y_pool = pl.pallas_call(
        state_kernel,
        grid=(steps,),
        in_specs=[
            moving(tile, width), fixed(halo_rows, width), fixed(*gain.shape),
            fixed(width, channels), fixed(width, channels), fixed(width, channels),
            fixed(*pool_mix.shape), fixed(1, channels), fixed(1, channels),
            pl.BlockSpec((heads, tile), lambda i: (0, i)),
        ],
        out_specs=[
            moving(tile, lanes), moving(tile, 3 * channels),
            moving(chunks, heads, head_k, head_k), moving(chunks, 8, channels),
            fixed(sp, heads * head_k + msg_pad, head_k),
        ] + [fixed(quarter, channels)] * tp,
        out_shape=[
            sds((rows, lanes), f32), sds((rows, 3 * channels), bf16),
            sds((rows // chunk, heads, head_k, head_k), bf16),
            sds((rows // chunk, 8, channels), f32),
            sds((sp, heads * head_k + msg_pad, head_k), bf16),
        ] + [sds((quarter, channels), bf16)] * tp,
        scratch_shapes=[
            pltpu.VMEM((width, 3 * channels), bf16), pltpu.VMEM((heads, head_k, head_k), f32),
            pltpu.VMEM((1, channels), f32), pltpu.VMEM((halo_rows, channels), bf16),
            pltpu.VMEM((chunk, chunk + halo_rows), bf16),
            pltpu.VMEM((tp, quarter, channels), bf16),
        ],
        compiler_params=limits(58),
        cost_estimate=pl.CostEstimate(
            flops=6 * rows * width * channels, transcendentals=0, bytes_accessed=2 * rows * width
        ),
        name="state_kernel",
    )(
        inputs, halo, gain, forget_weight, value_weight, pool_weight, pool_mix, pool_scale[None],
        lower_bound[None], extra_decay.T,
    )
    half = lax.dynamic_slice_in_dim(
        out_recur, (lax.axis_index("sp") % 2) * (channels // 2), channels // 2, axis=0
    )
    fetched = swapped(half, "tp", 2)
    handed = swapped(fetched, "sp", 1)
    cross_fetched = swapped(fetched, "tp", 1)
    cross_handed = swapped(handed, "tp", 1)
    w_recur = [
        [out_recur], [swapped(out_recur, "tp", 1)], [fetched, handed],
        [cross_fetched, cross_handed],
    ]


    def exchange(pieces):
        return [pieces[0]] + [swapped(pieces[k], "tp", k) for k in range(1, tp)]

    msgs = lax.all_to_all(msgs, "sp", split_axis=0, concat_axis=0, tiled=True)
    pool_seen = exchange(y_pool)
    parts = pl.pallas_call(
        local_kernel,
        grid=(steps,),
        in_specs=[
            moving(tile, width), fixed(*gain.shape), fixed(width, channels),
            fixed(width, channels), fixed(1, channels),
            moving(tile, lanes), moving(tile, 3 * channels),
            moving(chunks, heads, head_k, head_k), moving(chunks, 8, channels),
        ],
        out_specs=moving(tile, 3 * channels),
        out_shape=sds((rows, 3 * channels), bf16),
        scratch_shapes=[
            pltpu.VMEM((width, 2 * channels), bf16), pltpu.VMEM((6, channels, channels), bf16),
        ],
        compiler_params=limits(54),
        cost_estimate=pl.CostEstimate(
            flops=4 * rows * width * channels, transcendentals=0, bytes_accessed=2 * rows * width
        ),
        name="local_kernel",
    )(
        inputs, gain, query_weight, outgate_weight, recur_gain[None], scale, kept, starts, row_info,
    )

    def outputs(flip):
        part = pl.BlockSpec(
            (quarter, 3 * channels), lambda i: (lax.axis_index("tp") ^ (flip + i), 0)
        )
        return pl.pallas_call(
            output_kernel,
            grid=(2,),
            in_specs=[fixed(*msgs.shape), fixed(*init_state.shape), part],
            out_specs=[fixed(quarter, channels)] * 2,
            out_shape=[sds((quarter, channels), bf16)] * 2,
            scratch_shapes=[pltpu.VMEM((heads, head_k, head_k), bf16)],
            compiler_params=limits(40),
            cost_estimate=pl.CostEstimate(
                flops=2 * rows * head_k * channels, transcendentals=0,
                bytes_accessed=4 * rows * channels,
            ),
            name="output_kernel",
        )(msgs, init_state, parts)

    far_y = outputs(2)
    near_y = outputs(0)
    y_recur = near_y + far_y
    recur_seen = exchange(y_recur)
    partial_sum = project(pool_seen + recur_seen[:2], w_pool + w_recur[:2], None, bf16)
    return project(recur_seen[2:], w_recur[2:], partial_sum, bf16)


def solution(mesh):
    in_specs = (
        P("sp", None), P(), P(None, "tp"), P(None, "tp"), P(None, "tp"), P(None, "tp"),
        P(None, "tp"), P("tp", None, None), P("tp"), P("tp"), P("sp", "tp"), P("tp"),
        P("tp", None, None), P("tp", None), P("tp", None),
    )

    return jax.shard_map(
        per_device, mesh=mesh, in_specs=in_specs, out_specs=P(("sp", "tp"), None), check_vma=False
    )
```
